128 devices in a mesh: sp: 16 (over z, y), dp: 8 (over x, core).
Axes of the slice: x: 4, y: 4, z: 4, core: 2. Of those that a mesh axis runs over, the one named last changes fastest.
Arguments:
- queries: bfloat16 [8, 2048, 2048], P('dp', 'sp'), may hold values from -8 to 8
- keys: bfloat16 [8, 2048, 2048], P('dp', 'sp'), may hold values from -8 to 8
- values: bfloat16 [8, 2048, 2048], P('dp', 'sp'), may hold values from -6 to 6
- proj_weight: bfloat16 [2048, 2048], P('sp'), may hold values from -0.125 to 0.125
- residual: bfloat16 [8, 2048, 2048], P('dp', 'sp'), may hold values from -6 to 6
- norm_gain: float32 [2048], replicated, may hold values from 0.1 to 1.9
- route: int32 [8, 2048, 2], P('dp', 'sp'), may hold values from 0 to 15, all different within a row; in each aligned block of 128 rows (0 to 127, 128 to 255, ..., all dimensions but the last counted through in order) at most 32 rows name the same one
- route_weight: float32 [8, 2048, 2], P('dp', 'sp'), may hold values from 0.1 to 1
- w_gate: bfloat16 [16, 2048, 1024], P('sp'), may hold values from -0.125 to 0.125
- w_up: bfloat16 [16, 2048, 1024], P('sp'), may hold values from -0.125 to 0.125
- w_down: bfloat16 [16, 1024, 2048], P('sp'), may hold values from -0.1875 to 0.1875
Outputs:
- mixed: bfloat16 [8, 2048, 2048], P('dp', 'sp')
The draws below stay inside these ranges and needn't reach their ends.
Inputs may be any that keep to these rules, and one draw needn't show every extreme that they name: `route`: in the rows of one device no expert is named by more than 32 rows, a bound that some block reaches.
All inputs are finite; a program needn't handle non-finite values.
Results may differ from the reference program's by a relative error of at most 0.013.
Values may be sent and summed in bfloat16 or wider, within the bound.
A program may use at most 128 MiB of HBM per device.

```python
import math
import jax
import jax.numpy as jnp
import numpy as np
from jax import lax

D = 2048
HEADS = 16
HEAD_DIM = 128
FFE = 1024
SEQ_DEV = 128
EXPERTS = 16
LENGTH = 2048
SEQS = 8
CAP = 32
N_SP = 16
N_DP = 8


def head_plan(key):
    first, second, third = jax.random.split(jax.random.fold_in(key, 7), 3)
    direction = jnp.where(jax.random.bernoulli(first, 0.5, (HEADS, HEAD_DIM)), 1.0, -1.0).astype(jnp.float32)
    slow = jax.random.bernoulli(second, 0.5, (HEADS,))
    level = jnp.where(slow, -jnp.log(1.0 * LENGTH) - 1.5, -jnp.log(100.0))
    drift = jax.random.uniform(third, (SEQS, LENGTH // 64, HEADS), jnp.float32, -0.8, 0.8)
    drift = jnp.repeat(drift, 64, axis=1)
    return (direction, level[None, None, :] + drift)


def noise(key):
    sample = jnp.clip(jax.random.normal(key, (SEQS, LENGTH, HEADS, HEAD_DIM), jnp.float32), -6.0, 6.0)
    return sample


def draw_keys(key, part):
    direction, level = head_plan(key)
    sample = noise(jax.random.fold_in(key, 11)) + direction[None, None, :, :]
    return sample.reshape(SEQS, LENGTH, HEADS * HEAD_DIM).astype(jnp.bfloat16)


def draw_queries(key, part):
    direction, level = head_plan(key)
    factor = level / jnp.sqrt(1.0 * HEAD_DIM)
    sample = noise(jax.random.fold_in(key, 13)) + factor[..., None] * direction[None, None, :, :]
    return sample.reshape(SEQS, LENGTH, HEADS * HEAD_DIM).astype(jnp.bfloat16)


def shard_levels(own_key, extent, pieces, low, high):
    gain, own = 1.0, jax.random.fold_in(own_key, 6)
    for dim, blocks in pieces:
        heights = jnp.exp(jax.random.uniform(jax.random.fold_in(own, dim), (blocks,), jnp.float32, low / len(pieces), high / len(pieces)))
        gain = gain * jnp.repeat(heights, extent[dim] // blocks).reshape([-1 if axis == dim else 1 for axis in range(len(extent))])
    return gain


def assign_block(stream_key, own, number, rows, amount, top, most, lean):
    order = jax.random.permutation(stream_key, amount)
    packed, common = portions_of(amount, rows * top, most, lean, True), portions_of(amount, rows * top, most, lean, False)
    places = jnp.arange(amount)

    def named(sizes, offset_by):
        used = int((sizes > 0).sum())
        fixed = max(1, used // 4)
        passed = fixed + (places - fixed + offset_by * (used - fixed)) % max(1, amount - fixed)
        return jnp.zeros((amount,), jnp.int32).at[order[jnp.where(places < fixed, places, passed)]].set(jnp.asarray(sizes, jnp.int32))

    sizes = jnp.where(number % 4 == 0, named(packed, number // 4), named(common, number - number // 4 - 1))
    mixed = jax.random.permutation(jax.random.fold_in(own, 3), amount)
    giver, receiver = mixed[0:amount // 2 * 2:2], mixed[1:amount // 2 * 2:2]
    margin = jnp.minimum(sizes[giver] - 1, most - sizes[receiver]) // 2
    margin = jnp.where((giver == order[0]) | (receiver == order[0]) | (sizes[receiver] == 0), 0, jnp.maximum(margin, 0))
    passed = jax.random.randint(jax.random.fold_in(own, 4), (amount // 2,), 0, 1 << 20) % (margin + 1)
    sizes = sizes.at[giver].add(-passed).at[receiver].add(passed)
    items = jnp.searchsorted(jnp.cumsum(sizes), jnp.arange(rows * top), side="right").astype(jnp.int32)
    grid = items.reshape(top, rows).T
    grid = grid[jax.random.permutation(jax.random.fold_in(own, 1), rows)]
    offset_by = jax.random.randint(jax.random.fold_in(own, 2), (rows, 1), 0, top)
    return jnp.take_along_axis(grid, (jnp.arange(top)[None, :] + offset_by) % top, axis=1)


def portions_of(count, total, reach, skew, full):
    loads = [(1 << 20) // math.isqrt(standing ** skew) + 1 for standing in range(1, count + 1)]
    largest = reach if full else min(reach, max(-(-total // count), total * loads[0] // sum(loads)))
    least = 1 if total - largest >= count - 1 else 0
    holding, surplus = [largest] + [least] * (count - 1), total - largest - least * (count - 1)
    while surplus > 0:
        movable = [i for i in range(1, count) if holding[i] < largest] or [i for i in range(1, count) if holding[i] < reach]
        whole, budget = sum([loads[i] for i in movable]), surplus
        for i in movable:
            extra = min(reach - holding[i], max(1, budget * loads[i] // whole), surplus)
            holding[i] = holding[i] + extra
            surplus = surplus - extra
    return np.array(holding)


def bell_draw(rng, extent, spread, most, shards=(), held_as=jnp.bfloat16):
    drawn = spread * jax.random.normal(rng, extent, jnp.float32)
    if shards:
        drawn = drawn * shard_levels(rng, extent, shards, -0.22, 0.18)
    return jnp.clip(drawn, -most, most).astype(held_as)


def setup_inputs(seed: int = 0) -> dict:
    splits = jax.random.split(jax.random.key(seed), 12)
    queries = draw_queries(jax.random.fold_in(splits[11], 71), 0)
    keys = draw_keys(jax.random.fold_in(splits[11], 71), 0)
    values = bell_draw(splits[2], (SEQS, LENGTH, D), 1.0, 6.0, ((0, 8), (1, 16)))
    proj_weight = bell_draw(splits[3], (D, D), D ** -0.5, 0.125, ((0, 16),))
    residual = bell_draw(splits[4], (SEQS, LENGTH, D), 1.0, 6.0, ((0, 8), (1, 16)))
    norm_gain = jnp.clip(1.0 + 0.18 * jax.random.normal(splits[5], (D,), jnp.float32), 0.1, 1.9)
    route_keys = jax.random.split(jax.random.fold_in(splits[6], 1), SEQS * LENGTH // SEQ_DEV)
    route_turns = jax.random.permutation(jax.random.fold_in(splits[6], 3), SEQS * LENGTH // SEQ_DEV)
    route = jax.vmap(lambda own, number: assign_block(jax.random.fold_in(splits[6], 2), own, number, SEQ_DEV, EXPERTS, 2, CAP, 2))(route_keys, route_turns).reshape((SEQS, LENGTH, 2))
    route_weight = jnp.clip(0.1 + 0.9 * jax.random.uniform(splits[7], (SEQS, LENGTH, 2), jnp.float32) ** shard_levels(splits[7], (SEQS, LENGTH, 2), ((0, 8), (1, 16)), -0.2, 0.2), 0.1, 1.0)
    w_gate = bell_draw(splits[8], (EXPERTS, D, FFE), D ** -0.5, 0.125, ((0, 16),))
    w_up = bell_draw(splits[9], (EXPERTS, D, FFE), D ** -0.5, 0.125, ((0, 16),))
    w_down = bell_draw(splits[10], (EXPERTS, FFE, D), FFE ** -0.5, 0.1875, ((0, 16),))
    return {"queries": queries, "keys": keys, "values": values, "proj_weight": proj_weight, "residual": residual, "norm_gain": norm_gain, "route": route, "route_weight": route_weight, "w_gate": w_gate, "w_up": w_up, "w_down": w_down}


EPS = 1e-06

def one_head(args):
    query, key, value = args
    length = query.shape[0]
    scores = jnp.dot(query, key.T, preferred_element_type=jnp.float32) * HEAD_DIM ** (-0.5)
    position = jnp.arange(length)
    causal = position[None, :] < position[:, None]
    softer = jnp.where(causal, jax.nn.softplus(scores), 0.0)
    suffix = lax.cumsum(softer, axis=1, reverse=True)
    weight = jnp.exp(jnp.where(causal, scores - suffix, -jnp.inf)).astype(jnp.bfloat16)
    return jnp.dot(weight, value, preferred_element_type=jnp.float32).astype(jnp.bfloat16)

def by_heads(array):
    seqs, length, width = array.shape
    heads = width // HEAD_DIM
    return array.reshape(seqs, length, heads, HEAD_DIM).transpose(0, 2, 1, 3).reshape(seqs * heads, length, HEAD_DIM)

def reference(queries, keys, values, proj_weight, residual, norm_gain, route, route_weight, w_gate, w_up, w_down):
    seqs, length, width = queries.shape
    heads = width // HEAD_DIM
    attended = lax.map(one_head, (by_heads(queries), by_heads(keys), by_heads(values)))
    attended = attended.reshape(seqs, heads, length, HEAD_DIM).transpose(0, 2, 1, 3).reshape(seqs * length, width)
    projected = jnp.dot(attended, proj_weight, preferred_element_type=jnp.float32)
    stream = (residual.reshape(seqs * length, width).astype(jnp.float32) + projected).astype(jnp.bfloat16)
    stream_f = stream.astype(jnp.float32)
    normed = (stream_f * lax.rsqrt(lax.optimization_barrier(jnp.mean(stream_f * stream_f, axis=-1, keepdims=True)) + EPS) * norm_gain).astype(jnp.bfloat16)
    flat_route = route.reshape(seqs * length, 2)
    flat_weight = route_weight.reshape(seqs * length, 2)
    bound = CAP * N_SP * N_DP

    def per_expert(total, inputs):
        expert, gate_w, up_w, down_w = inputs
        named = flat_route == expert
        scale = lax.optimization_barrier(jnp.sum(jnp.where(named, flat_weight, 0.0), axis=1))
        used = jnp.any(named, axis=1)
        index = jnp.nonzero(used, size=bound, fill_value=0)[0]
        valid = jnp.arange(bound) < jnp.sum(used.astype(jnp.int32))
        rows = normed[index]
        gate = jnp.dot(rows, gate_w, preferred_element_type=jnp.float32)
        upper = jnp.dot(rows, up_w, preferred_element_type=jnp.float32)
        hidden = (jax.nn.silu(gate) * upper).astype(jnp.bfloat16)
        result = jnp.dot(hidden, down_w, preferred_element_type=jnp.float32).astype(jnp.bfloat16)
        addend = jnp.where(valid[:, None], scale[index][:, None] * result.astype(jnp.float32), 0.0)
        return (total.at[index].add(addend), None)
    experts = w_gate.shape[0]
    total, unused = lax.scan(per_expert, stream.astype(jnp.float32), (jnp.arange(experts).astype(jnp.int32), w_gate, w_up, w_down))
    return total.astype(jnp.bfloat16).reshape(seqs, length, width)
```

```python
import functools
import math

import jax
import jax.numpy as jnp
from jax import lax
from jax.experimental import pallas as pl
from jax.experimental.pallas import tpu as pltpu
from jax.sharding import PartitionSpec as P

MESH = pl.DeviceIdType.MESH
EPS = 1e-06
SIDE = 4
N_SP = 16
ROWS = 128
HEAD = 128
LENGTH = 2048
WIDTH = 2048
FFE = 1024
CAP = 32
TILE = 256
LOG2E = 1.0 / math.log(2.0)

SHIFTS = (
    (1, 2), (3, 2), (2, 1), (2, 3),
    (2, 2), (2, 0), (0, 2), (0, 0),
    (1, 1), (3, 3), (1, 3), (3, 1),
    (1, 0), (3, 0), (0, 1), (0, 3),
)
OWN = SHIFTS.index((0, 0))
GROUPS = 4
PER_GROUP = 4
GROUP_ROWS = PER_GROUP * CAP


def dot(a, b):
    return jnp.dot(a, b, preferred_element_type=jnp.float32)


def body_kernel(
    q_hbm, k_hbm, v_hbm, proj_hbm, res_hbm, gain_ref, route_ref, rw_ref,
    wg_hbm, wu_hbm, wd_hbm,
    out_ref,
    qh, kh, vh, w_att, carry, tri, o_buf, oa, ob, proj_a, proj_b,
    part_a, part_b, sum_a, sum_b, res, acc, normed, pick, mix_hi, mix_lo,
    xs, xr, ys, yr, hid, wg, wu, wd,
    local_sem, head_send, head_recv, proj_send, proj_recv, o_send, o_recv,
    r_send, r_recv, d_send, d_recv, y_send, y_recv,
):
    me = lax.axis_index("sp")
    z = me // SIDE
    y = me % SIDE

    def at(a, b):
        return ((z + a) % SIDE) * SIDE + (y + b) % SIDE

    others = [s for s in SHIFTS if s != (0, 0)]
    line = (2, 1, 3)

    barrier = pltpu.get_barrier_semaphore()
    for a, b in others:
        pl.semaphore_signal(barrier, inc=1, device_id={"sp": at(a, b)}, device_id_type=MESH)

    def local(src, dst, sem):
        copy = pltpu.make_async_copy(src, dst, sem)
        copy.start()
        return copy

    def remote(src, dst, send, recv, peer):
        pltpu.make_async_remote_copy(
            src_ref=src, dst_ref=dst, send_sem=send, recv_sem=recv,
            device_id={"sp": peer}, device_id_type=MESH,
        ).start()

    def wait_for(ref, sem):
        pltpu.make_async_copy(ref, ref, sem).wait()

    my_rows = pl.ds(pl.multiple_of(me * ROWS, ROWS), ROWS)

    def cols(peer):
        return pl.ds(pl.multiple_of(peer * HEAD, HEAD), HEAD)

    heads = ((k_hbm, kh), (q_hbm, qh), (v_hbm, vh))
    for t, (src, dst) in enumerate(heads):
        local(src.at[0, :, cols(me)], dst.at[my_rows], head_recv.at[t])
    local(proj_hbm.at[:, pl.ds(0, 1024)], proj_a.at[y], proj_recv.at[0])
    local(proj_hbm.at[:, pl.ds(1024, 1024)], proj_b.at[z], proj_recv.at[1])

    pl.semaphore_wait(barrier, N_SP - 1)

    def send_heads(t, a, b):
        src, dst = heads[t]
        peer = at(a, b)
        remote(src.at[0, :, cols(peer)], dst.at[my_rows], head_send.at[t], head_recv.at[t], peer)

    for a, b in others:
        send_heads(0, a, b)
        send_heads(1, a, b)
    for a, b in others:
        send_heads(2, a, b)
    for s in line:
        remote(proj_hbm.at[:, pl.ds(0, 1024)], proj_a.at[y], proj_send.at[0], proj_recv.at[0], at(0, s))
        remote(proj_hbm.at[:, pl.ds(1024, 1024)], proj_b.at[z], proj_send.at[1], proj_recv.at[1], at(s, 0))
    loads = [
        local(res_hbm.at[0], res, local_sem.at[0]),
        local(wg_hbm.at[0], wg, local_sem.at[1]),
        local(wu_hbm.at[0], wu, local_sem.at[2]),
        local(wd_hbm.at[0], wd, local_sem.at[3]),
    ]

    j = lax.broadcasted_iota(jnp.int32, (TILE, TILE + HEAD), 0)
    s = lax.broadcasted_iota(jnp.int32, (TILE, TILE + HEAD), 1)
    tri[...] = jnp.where((j > s) | (s >= TILE), 1.0, 0.0).astype(jnp.bfloat16)

    @pl.loop(0, LENGTH // 64)
    def _(i):
        w_att[pl.ds(pl.multiple_of(i * 64, 64), 64), :] = jnp.zeros((64, LENGTH), jnp.bfloat16)

    slots = N_SP * CAP
    lane = lax.broadcasted_iota(jnp.int32, (ROWS, slots), 1)
    place = lane // CAP
    expert = jnp.zeros((ROWS, slots), jnp.int32)
    for i, (a, b) in enumerate(SHIFTS):
        expert = jnp.where(place == i, at(a, b), expert)
    first = route_ref[0, :, 0:1] == expert
    second = route_ref[0, :, 1:2] == expert
    named = jnp.where(first | second, 1.0, 0.0)
    r0 = lax.broadcasted_iota(jnp.int32, (ROWS, ROWS), 0)
    r1 = lax.broadcasted_iota(jnp.int32, (ROWS, ROWS), 1)
    before = jnp.where(r1 < r0, 1.0, 0.0).astype(jnp.bfloat16)
    slot = dot(before, named.astype(jnp.bfloat16))
    held = jnp.where(slot == (lane - place * CAP).astype(jnp.float32), named, 0.0)
    pick[...] = held.T.astype(jnp.bfloat16)
    mix = held * jnp.where(first, rw_ref[0, :, 0:1], rw_ref[0, :, 1:2])
    high = mix.astype(jnp.bfloat16)
    mix_hi[...] = high
    mix_lo[...] = (mix - high.astype(jnp.float32)).astype(jnp.bfloat16)

    wait_for(kh, head_recv.at[0])
    wait_for(qh, head_recv.at[1])
    scale = HEAD ** (-0.5) * LOG2E

    def weights(q0, k0, diagonal):
        q_rows = pl.ds(q0, TILE)
        k_rows = pl.ds(k0, TILE)
        u = lax.dot_general(
            qh[q_rows, :], kh[k_rows, :], (((1,), (1,)), ((), ())),
            preferred_element_type=jnp.float32,
        ) * scale
        low = jnp.log(1.0 + jnp.exp2(-jnp.abs(u))) * LOG2E
        soft = jnp.maximum(u, 0.0) + low
        if diagonal:
            causal = lax.broadcasted_iota(jnp.int32, (TILE, TILE), 1) < lax.broadcasted_iota(
                jnp.int32, (TILE, TILE), 0
            )
            soft = jnp.where(causal, soft, 0.0)
        sums = dot(soft.astype(jnp.bfloat16), tri[...])
        power = jnp.minimum(u, 0.0) - low - sums[:, :TILE]
        total = sums[:, TILE:]
        if not diagonal:
            later = carry[q_rows, :]
            power = power - jnp.concatenate([later, later], axis=1)
            total = total + later
        weight = jnp.exp2(power)
        if diagonal:
            weight = jnp.where(causal, weight, 0.0)
        w_att[q_rows, k_rows] = weight.astype(jnp.bfloat16)
        carry[q_rows, :] = total

    @pl.loop(0, 4)
    def _(i):
        for half in range(2):
            base = pl.multiple_of(i * 512 + half * TILE, TILE)
            weights(base, base, True)

    @pl.loop(0, 2)
    def _(i):
        for half in range(2):
            base = pl.multiple_of(i * 1024 + half * 512, TILE)
            weights(base + TILE, base, False)

    for big in range(1, 4):
        @pl.loop(0, 2 * big)
        def _(i):
            k0 = pl.multiple_of((2 * big - 1 - i) * TILE, TILE)
            for half in range(2):
                weights(big * 512 + half * TILE, k0, False)

    wait_for(vh, head_recv.at[2])
    for i in range(SIDE):
        quarter = (z + 1 + i) % SIDE
        rows = pl.ds(pl.multiple_of(quarter * 512, 512), 512)
        o_buf[quarter] = dot(w_att[rows, :], vh[...]).astype(jnp.bfloat16).reshape(SIDE, ROWS, HEAD)
        if i < SIDE - 1:
            remote(o_buf.at[quarter], ob.at[:, :, cols(z)], o_send.at[1], o_recv.at[1], quarter * SIDE + y)
    for s in line:
        peer_y = (y + s) % SIDE
        remote(o_buf.at[:, peer_y], oa.at[:, :, cols(y)], o_send.at[0], o_recv.at[0], z * SIDE + peer_y)
    ob[:, :, cols(z)] = o_buf[z]
    for i in range(SIDE):
        oa[i, :, cols(y)] = o_buf[i, y]

    def project(index, o_in, weight, part):
        wait_for(weight, proj_recv.at[index])
        wait_for(o_in.at[:, :, pl.ds(0, 3 * HEAD)], o_recv.at[index])
        left = o_in[...].reshape(512, 512)

        @pl.loop(0, 1024 // TILE)
        def _(n):
            c = pl.ds(pl.multiple_of(n * TILE, TILE), TILE)
            right = weight[:, :, c].reshape(512, TILE)
            part[:, :, c] = dot(left, right).astype(jnp.bfloat16).reshape(SIDE, ROWS, TILE)

    project(1, ob, proj_b, part_b)
    for s in line:
        peer_y = (y + s) % SIDE
        remote(part_b.at[peer_y], sum_b.at[y], r_send.at[1], r_recv.at[1], z * SIDE + peer_y)
    project(0, oa, proj_a, part_a)
    for s in line:
        peer_z = (z + s) % SIDE
        remote(part_a.at[peer_z], sum_a.at[z], r_send.at[0], r_recv.at[0], peer_z * SIDE + y)
    sum_b[y] = part_b[y]
    sum_a[z] = part_a[z]
    loads[0].wait()
    wait_for(sum_b.at[pl.ds(0, 3)], r_recv.at[1])
    wait_for(sum_a.at[pl.ds(0, 3)], r_recv.at[0])

    @pl.loop(0, ROWS // 16)
    def _(i):
        r = pl.ds(pl.multiple_of(i * 16, 16), 16)
        halves = []
        for h, sums in enumerate((sum_a, sum_b)):
            total = res[r, h * 1024:(h + 1) * 1024].astype(jnp.float32)
            for k in range(SIDE):
                total = total + sums[k, r, :].astype(jnp.float32)
            halves.append(total.astype(jnp.bfloat16).astype(jnp.float32))
        stream = jnp.concatenate(halves, axis=1)
        acc[r, :] = stream
        mean = jnp.mean(stream * stream, axis=-1, keepdims=True)
        normed[r, :] = (stream * lax.rsqrt(mean + EPS) * gain_ref[...]).astype(jnp.bfloat16)

    for g in range(GROUPS):
        @pl.loop(0, WIDTH // 512)
        def _(n):
            c = pl.ds(pl.multiple_of(n * 512, 512), 512)
            rows = dot(pick[g * GROUP_ROWS:(g + 1) * GROUP_ROWS, :], normed[:, c])
            rows = rows.astype(jnp.bfloat16).reshape(PER_GROUP, CAP, 512)
            xs[g * PER_GROUP:(g + 1) * PER_GROUP, :, c] = rows

        for i in range(g * PER_GROUP, (g + 1) * PER_GROUP):
            if i == OWN:
                xr[i] = xs[i]
            else:
                remote(xs.at[i], xr.at[i], d_send, d_recv.at[g], at(*SHIFTS[i]))

    loads[1].wait()
    loads[2].wait()
    loads[3].wait()

    def remote_count(g):
        return PER_GROUP - (1 if OWN // PER_GROUP == g else 0)

    for g in range(GROUPS):
        mine = slice(g * PER_GROUP, (g + 1) * PER_GROUP)
        wait_for(xr.at[pl.ds(g * PER_GROUP, remote_count(g))], d_recv.at[g])

        @pl.loop(0, FFE // TILE)
        def _(n):
            c = pl.ds(pl.multiple_of(n * TILE, TILE), TILE)
            x = xr[mine].reshape(GROUP_ROWS, WIDTH)
            gate = dot(x, wg[:, c])
            upper = dot(x, wu[:, c])
            hid[:, c] = (gate / (1.0 + jnp.exp(-gate)) * upper).astype(jnp.bfloat16)

        @pl.loop(0, WIDTH // 512)
        def _(n):
            c = pl.ds(pl.multiple_of(n * 512, 512), 512)
            result = dot(hid[...], wd[:, c]).astype(jnp.bfloat16)
            ys[mine, :, c] = result.reshape(PER_GROUP, CAP, 512)

        for i in range(g * PER_GROUP, (g + 1) * PER_GROUP):
            if i == OWN:
                yr[i] = ys[i]
            else:
                a, b = SHIFTS[i]
                remote(ys.at[i], yr.at[i], y_send, y_recv.at[g], at(-a, -b))

    for g in range(GROUPS):
        wait_for(yr.at[pl.ds(g * PER_GROUP, remote_count(g))], y_recv.at[g])

        @pl.loop(0, WIDTH // 512)
        def _(n):
            c = pl.ds(pl.multiple_of(n * 512, 512), 512)
            lanes = slice(g * GROUP_ROWS, (g + 1) * GROUP_ROWS)
            got = yr[g * PER_GROUP:(g + 1) * PER_GROUP, :, c].reshape(GROUP_ROWS, 512)
            total = acc[:, c] + dot(mix_hi[:, lanes], got) + dot(mix_lo[:, lanes], got)
            if g < GROUPS - 1:
                acc[:, c] = total
            else:
                out_ref[0, :, c] = total.astype(jnp.bfloat16)

    fifteen = pl.ds(0, N_SP - 1)
    for t, (src, dst) in enumerate(heads):
        wait_for(dst.at[pl.ds(0, ROWS * (N_SP - 1))], head_send.at[t])
    for i in range(2):
        wait_for(proj_a.at[pl.ds(0, 3)], proj_send.at[i])
        wait_for(o_buf.at[pl.ds(0, 3)], o_send.at[i])
        wait_for(part_a.at[pl.ds(0, 3)], r_send.at[i])
    wait_for(xs.at[fifteen], d_send)
    wait_for(ys.at[fifteen], y_send)


def body(
    queries, keys, values, proj_weight, residual, norm_gain, route, route_weight,
    w_gate, w_up, w_down,
):
    bf16, f32 = jnp.bfloat16, jnp.float32
    vmem = pltpu.VMEM
    dma = pltpu.SemaphoreType.DMA
    anywhere = pl.BlockSpec(memory_space=pl.ANY)
    inside = pl.BlockSpec(memory_space=pltpu.VMEM)
    scratch = [
        vmem((LENGTH, HEAD), bf16), vmem((LENGTH, HEAD), bf16), vmem((LENGTH, HEAD), bf16),
        vmem((LENGTH, LENGTH), bf16), vmem((LENGTH, HEAD), f32), vmem((TILE, TILE + HEAD), bf16),
        vmem((SIDE, SIDE, ROWS, HEAD), bf16),
        vmem((SIDE, ROWS, 512), bf16), vmem((SIDE, ROWS, 512), bf16),
        vmem((SIDE, ROWS, 1024), bf16), vmem((SIDE, ROWS, 1024), bf16),
        vmem((SIDE, ROWS, 1024), bf16), vmem((SIDE, ROWS, 1024), bf16),
        vmem((SIDE, ROWS, 1024), bf16), vmem((SIDE, ROWS, 1024), bf16),
        vmem((ROWS, WIDTH), bf16), vmem((ROWS, WIDTH), f32), vmem((ROWS, WIDTH), bf16),
        vmem((N_SP * CAP, ROWS), bf16), vmem((ROWS, N_SP * CAP), bf16), vmem((ROWS, N_SP * CAP), bf16),
        vmem((N_SP, CAP, WIDTH), bf16), vmem((N_SP, CAP, WIDTH), bf16),
        vmem((N_SP, CAP, WIDTH), bf16), vmem((N_SP, CAP, WIDTH), bf16),
        vmem((GROUP_ROWS, FFE), bf16),
        vmem((WIDTH, FFE), bf16), vmem((WIDTH, FFE), bf16), vmem((FFE, WIDTH), bf16),
        dma((4,)), dma((3,)), dma((3,)), dma((2,)), dma((2,)), dma((2,)), dma((2,)),
        dma((2,)), dma((2,)), dma, dma((GROUPS,)), dma, dma((GROUPS,)),
    ]
    return pl.pallas_call(
        body_kernel,
        out_shape=jax.ShapeDtypeStruct((1, ROWS, WIDTH), bf16),
        in_specs=[anywhere] * 5 + [inside] * 3 + [anywhere] * 3,
        out_specs=inside,
        scratch_shapes=scratch,
        compiler_params=pltpu.CompilerParams(
            collective_id=0, has_side_effects=True, vmem_limit_bytes=62 * 1024 * 1024
        ),
        name="layer",
    )(
        queries, keys, values, proj_weight, residual, norm_gain.reshape(1, WIDTH), route,
        route_weight, w_gate, w_up, w_down,
    )


def solution(mesh):
    return jax.shard_map(
        body,
        mesh=mesh,
        in_specs=(
            P("dp", "sp", None),
            P("dp", "sp", None),
            P("dp", "sp", None),
            P("sp", None),
            P("dp", "sp", None),
            P(),
            P("dp", "sp", None),
            P("dp", "sp", None),
            P("sp", None, None),
            P("sp", None, None),
            P("sp", None, None),
        ),
        out_specs=P("dp", "sp", None),
        check_vma=False,
    )
```

```python
import functools
import math

import jax
import jax.numpy as jnp
from jax import lax
from jax.experimental import pallas as pl
from jax.experimental.pallas import tpu as pltpu
from jax.sharding import PartitionSpec as P

MESH = pl.DeviceIdType.MESH
EPS = 1e-06
SIDE = 4
N_SP = 16
ROWS = 128
HEAD = 128
LENGTH = 2048
WIDTH = 2048
FFE = 1024
HALF = 1024
CHUNK = 512
CHUNKS = 4
CAP = 32
TILE = 256
LOG2E = 1.0 / math.log(2.0)

SHIFTS = (
    (1, 2), (3, 2), (2, 1), (2, 3),
    (2, 2), (2, 0), (0, 2), (0, 0),
    (1, 1), (3, 3), (1, 3), (3, 1),
    (1, 0), (3, 0), (0, 1), (0, 3),
)
OWN = SHIFTS.index((0, 0))
GROUPS = 4
PER_GROUP = 4
GROUP_ROWS = PER_GROUP * CAP


def dot(a, b):
    return jnp.dot(a, b, preferred_element_type=jnp.float32)


def body_kernel(
    q_hbm, k_hbm, v_hbm, proj_hbm, res_hbm, gain_ref, route_ref, rw_ref,
    wg_hbm, wu_hbm, wd_hbm,
    out_ref,
    qh, kh, vh, w_att, carry, tri, o_buf, oa, ob, proj_a, proj_b,
    part_a, part_b, sum_a, sum_b, res, acc, pick, mix_hi, mix_lo,
    xs, xr, ys, yr, scaled, squares, gate_acc, up_acc, hid, wg, wu, wd,
    local_sem, head_send, head_recv, proj_send, proj_recv, relay_send, relay_recv,
    o_send, oa_recv, ob_recv, r_send, ra_recv, rb_recv, d_send, d_recv, y_send, y_recv,
):
    me = lax.axis_index("sp")
    dp = lax.axis_index("dp")
    z = me // SIDE
    y = me % SIDE
    core = dp % 2
    partner = dp + 1 - 2 * core

    def at(a, b):
        return ((z + a) % SIDE) * SIDE + (y + b) % SIDE

    others = [s for s in SHIFTS if s != (0, 0)]
    line = (2, 1, 3)

    barrier = pltpu.get_barrier_semaphore()
    for a, b in others:
        pl.semaphore_signal(barrier, inc=1, device_id={"sp": at(a, b)}, device_id_type=MESH)
    pl.semaphore_signal(barrier, inc=1, device_id={"dp": partner}, device_id_type=MESH)

    def local(src, dst, sem):
        copy = pltpu.make_async_copy(src, dst, sem)
        copy.start()
        return copy

    def remote(src, dst, send, recv, peer, axis="sp"):
        pltpu.make_async_remote_copy(
            src_ref=src, dst_ref=dst, send_sem=send, recv_sem=recv,
            device_id={axis: peer}, device_id_type=MESH,
        ).start()

    def wait_for(ref, sem):
        pltpu.make_async_copy(ref, ref, sem).wait()

    my_rows = pl.ds(pl.multiple_of(me * ROWS, ROWS), ROWS)
    core_rows = pl.ds(pl.multiple_of(core * (ROWS // 2), ROWS // 2), ROWS // 2)

    def cols(peer):
        return pl.ds(pl.multiple_of(peer * HEAD, HEAD), HEAD)

    heads = ((k_hbm, kh), (q_hbm, qh), (v_hbm, vh))
    for t, (src, dst) in enumerate(heads):
        local(src.at[0, :, cols(me)], dst.at[my_rows], head_recv.at[t])
    loads = [
        local(proj_hbm.at[:, pl.ds(0, HALF)], proj_a.at[y], local_sem.at[4]),
        local(proj_hbm.at[:, pl.ds(HALF, HALF)], proj_b.at[z], local_sem.at[5]),
    ]

    pl.semaphore_wait(barrier, N_SP)

    def send_heads(t, a, b):
        src, dst = heads[t]
        peer = at(a, b)
        remote(src.at[0, :, cols(peer)], dst.at[my_rows], head_send.at[t], head_recv.at[t], peer)

    for a, b in others:
        send_heads(0, a, b)
        send_heads(1, a, b)
    for a, b in others:
        send_heads(2, a, b)
    for s in line:
        remote(proj_hbm.at[core_rows, pl.ds(0, HALF)], proj_a.at[y, core_rows],
               proj_send.at[0], proj_recv.at[0], at(0, s))
    for s in line:
        remote(proj_hbm.at[core_rows, pl.ds(HALF, HALF)], proj_b.at[z, core_rows],
               proj_send.at[1], proj_recv.at[1], at(s, 0))
    loads += [
        local(res_hbm.at[0], res, local_sem.at[0]),
        local(wg_hbm.at[0], wg, local_sem.at[1]),
        local(wu_hbm.at[0], wu, local_sem.at[2]),
        local(wd_hbm.at[0], wd, local_sem.at[3]),
    ]

    j = lax.broadcasted_iota(jnp.int32, (TILE, TILE + HEAD), 0)
    s = lax.broadcasted_iota(jnp.int32, (TILE, TILE + HEAD), 1)
    tri[...] = jnp.where((j > s) | (s >= TILE), 1.0, 0.0).astype(jnp.bfloat16)

    @pl.loop(0, LENGTH // 64)
    def _(i):
        w_att[pl.ds(pl.multiple_of(i * 64, 64), 64), :] = jnp.zeros((64, LENGTH), jnp.bfloat16)

    slots = N_SP * CAP
    lane = lax.broadcasted_iota(jnp.int32, (ROWS, slots), 1)
    place = lane // CAP
    expert = jnp.zeros((ROWS, slots), jnp.int32)
    for i, (a, b) in enumerate(SHIFTS):
        expert = jnp.where(place == i, at(a, b), expert)
    zeros = jnp.zeros((6, ROWS), jnp.float32)
    route = jnp.concatenate([route_ref[0].astype(jnp.float32), zeros], axis=0).T
    share = jnp.concatenate([rw_ref[0], zeros], axis=0).T
    expert = expert.astype(jnp.float32)
    first = route[:, 0:1] == expert
    second = route[:, 1:2] == expert
    named = jnp.where(first | second, 1.0, 0.0)
    r0 = lax.broadcasted_iota(jnp.int32, (ROWS, ROWS), 0)
    r1 = lax.broadcasted_iota(jnp.int32, (ROWS, ROWS), 1)
    before = jnp.where(r1 < r0, 1.0, 0.0).astype(jnp.bfloat16)
    slot = dot(before, named.astype(jnp.bfloat16))
    held = jnp.where(slot == (lane - place * CAP).astype(jnp.float32), named, 0.0)
    pick[...] = held.T.astype(jnp.bfloat16)
    mix = held * jnp.where(first, share[:, 0:1], share[:, 1:2])
    high = mix.astype(jnp.bfloat16)
    mix_hi[...] = high
    mix_lo[...] = (mix - high.astype(jnp.float32)).astype(jnp.bfloat16)

    wait_for(kh, head_recv.at[0])
    wait_for(qh, head_recv.at[1])
    scale = HEAD ** (-0.5) * LOG2E

    def weights(q0, k0, diagonal):
        q_rows = pl.ds(q0, TILE)
        k_rows = pl.ds(k0, TILE)
        u = lax.dot_general(
            qh[q_rows, :], kh[k_rows, :], (((1,), (1,)), ((), ())),
            preferred_element_type=jnp.float32,
        ) * scale
        low = jnp.log(1.0 + jnp.exp2(-jnp.abs(u))) * LOG2E
        soft = jnp.maximum(u, 0.0) + low
        if diagonal:
            causal = lax.broadcasted_iota(jnp.int32, (TILE, TILE), 1) < lax.broadcasted_iota(
                jnp.int32, (TILE, TILE), 0
            )
            soft = jnp.where(causal, soft, 0.0)
        sums = dot(soft.astype(jnp.bfloat16), tri[...])
        power = jnp.minimum(u, 0.0) - low - sums[:, :TILE]
        total = sums[:, TILE:]
        if not diagonal:
            later = carry[q_rows, :]
            power = power - jnp.concatenate([later, later], axis=1)
            total = total + later
        weight = jnp.exp2(power)
        if diagonal:
            weight = jnp.where(causal, weight, 0.0)
        w_att[q_rows, k_rows] = weight.astype(jnp.bfloat16)
        carry[q_rows, :] = total

    @pl.loop(0, 4)
    def _(i):
        for half in range(2):
            base = pl.multiple_of(i * 512 + half * TILE, TILE)
            weights(base, base, True)

    @pl.loop(0, 2)
    def _(i):
        for half in range(2):
            base = pl.multiple_of(i * 1024 + half * 512, TILE)
            weights(base + TILE, base, False)

    for big in range(1, 4):
        @pl.loop(0, 2 * big)
        def _(i):
            k0 = pl.multiple_of((2 * big - 1 - i) * TILE, TILE)
            for half in range(2):
                weights(big * 512 + half * TILE, k0, False)

    wait_for(vh, head_recv.at[2])
    for i in range(SIDE):
        quarter = (z + 1 + i) % SIDE
        rows = pl.ds(pl.multiple_of(quarter * 512, 512), 512)
        o_buf[quarter] = dot(w_att[rows, :], vh[...]).astype(jnp.bfloat16).reshape(SIDE, ROWS, HEAD)
        if i < SIDE - 1:
            remote(o_buf.at[quarter], ob.at[:, :, cols(z)], o_send.at[1], ob_recv, quarter * SIDE + y)
        else:
            ob[:, :, cols(z)] = o_buf[z]
        for s in line:
            peer_y = (y + s) % SIDE
            remote(o_buf.at[quarter, peer_y], oa.at[quarter, :, cols(y)], o_send.at[0],
                   oa_recv.at[quarter], z * SIDE + peer_y)
        oa[quarter, :, cols(y)] = o_buf[quarter, y]

    three = pl.ds(0, SIDE - 1)
    half_rows = pl.ds(0, ROWS // 2)
    for index, (weight, mine) in enumerate(((proj_a, y), (proj_b, z))):
        wait_for(weight.at[three, half_rows], proj_recv.at[index])
        for s in line:
            piece = weight.at[(mine + s) % SIDE, core_rows]
            remote(piece, piece, relay_send.at[index], relay_recv.at[index], partner, "dp")

    loads[0].wait()
    wait_for(proj_a.at[three, half_rows], relay_recv.at[0])
    for i in range(SIDE):
        quarter = (z + 1 + i) % SIDE
        wait_for(oa.at[0, :, pl.ds(0, 3 * HEAD)], oa_recv.at[quarter])
        left = oa[quarter]
        for q in range(2):
            for n in range(2):
                c = slice(q * CHUNK + n * TILE, q * CHUNK + (n + 1) * TILE)
                right = proj_a[:, :, c].reshape(512, TILE)
                part_a[q, quarter, :, n * TILE:(n + 1) * TILE] = dot(left, right).astype(jnp.bfloat16)
        if i < SIDE - 1:
            remote(part_a.at[0, quarter], sum_a.at[0, z], r_send.at[0], ra_recv.at[0], quarter * SIDE + y)
    for s in (1, 2, 3):
        peer_z = (z + s) % SIDE
        remote(part_a.at[1, peer_z], sum_a.at[1, z], r_send.at[0], ra_recv.at[1], peer_z * SIDE + y)
    loads[1].wait()
    wait_for(proj_b.at[three, half_rows], relay_recv.at[1])
    wait_for(ob.at[:, :, pl.ds(0, 3 * HEAD)], ob_recv)
    for q in range(2):
        @pl.loop(0, 2)
        def _(n):
            c = pl.ds(pl.multiple_of(q * CHUNK + n * TILE, TILE), TILE)
            right = proj_b[:, :, c].reshape(512, TILE)
            block = dot(ob[...].reshape(512, 512), right).astype(jnp.bfloat16)
            part_b[q, :, :, pl.ds(pl.multiple_of(n * TILE, TILE), TILE)] = block.reshape(SIDE, ROWS, TILE)

        for s in line:
            peer_y = (y + s) % SIDE
            remote(part_b.at[q, peer_y], sum_b.at[q, y], r_send.at[1], rb_recv.at[q], z * SIDE + peer_y)
    for q in range(2):
        sum_a[q, z] = part_a[q, z]
        sum_b[q, y] = part_b[q, y]

    pieces = ((sum_a, ra_recv, 0, 0), (sum_b, rb_recv, 0, HALF),
              (sum_a, ra_recv, 1, CHUNK), (sum_b, rb_recv, 1, HALF + CHUNK))
    loads[2].wait()
    for k, (sums, recv, q, start) in enumerate(pieces):
        wait_for(sums.at[q, three], recv.at[q])
        total = res[:, start:start + CHUNK].astype(jnp.float32)
        for i in range(SIDE):
            total = total + sums[q, i].astype(jnp.float32)
        stream = total.astype(jnp.bfloat16)
        acc[:, start:start + CHUNK] = stream.astype(jnp.float32)
        for n in range(2):
            c = slice(n * TILE, (n + 1) * TILE)
            rows = dot(pick[...], stream[:, c]).astype(jnp.bfloat16)
            xs[k, :, :, c] = rows.reshape(N_SP, CAP, TILE)
        for i, (a, b) in enumerate(SHIFTS):
            if i != OWN:
                sem = d_recv.at[k] if k < CHUNKS - 1 else d_recv.at[k + i // PER_GROUP]
                remote(xs.at[k, i], xr.at[k, i], d_send, sem, at(a, b))
        xr[k, OWN] = xs[k, OWN]

    for load in loads[3:]:
        load.wait()
    fifteen = pl.ds(0, N_SP - 1)
    for k in range(CHUNKS - 1):
        start = pieces[k][3]
        wait_for(xr.at[k, fifteen], d_recv.at[k])

        @pl.loop(0, N_SP // 2)
        def _(i):
            rows = xr[k, pl.ds(2 * i, 2)].astype(jnp.float32).reshape(2 * CAP, CHUNK)
            r = pl.ds(pl.multiple_of(i * 2 * CAP, 2 * CAP), 2 * CAP)
            scaled[r, :] = (rows * gain_ref[:, start:start + CHUNK]).astype(jnp.bfloat16)
            square = jnp.sum(rows * rows, axis=-1, keepdims=True)
            square = jnp.broadcast_to(square, (2 * CAP, HEAD))
            squares[r, :] = square if k == 0 else squares[r, :] + square

        @pl.loop(0, FFE // TILE)
        def _(n):
            c = pl.ds(pl.multiple_of(n * TILE, TILE), TILE)
            for weight, total in ((wg, gate_acc), (wu, up_acc)):
                new = dot(scaled[...], weight[start:start + CHUNK, c])
                total[:, c] = new if k == 0 else total[:, c] + new

    def remote_count(g):
        return PER_GROUP - (1 if OWN // PER_GROUP == g else 0)

    last = CHUNKS - 1
    start = pieces[last][3]
    for g in range(GROUPS):
        mine = slice(g * PER_GROUP, (g + 1) * PER_GROUP)
        lines = slice(g * GROUP_ROWS, (g + 1) * GROUP_ROWS)
        wait_for(xr.at[last, pl.ds(g * PER_GROUP, remote_count(g))], d_recv.at[last + g])
        rows = xr[last, mine].astype(jnp.float32).reshape(GROUP_ROWS, CHUNK)
        scaled[lines, :] = (rows * gain_ref[:, start:start + CHUNK]).astype(jnp.bfloat16)
        square = squares[lines, 0:1] + jnp.sum(rows * rows, axis=-1, keepdims=True)
        factor = lax.rsqrt(square * (1.0 / WIDTH) + EPS)
        squares[lines, :] = jnp.broadcast_to(factor, (GROUP_ROWS, HEAD))

        @pl.loop(0, FFE // TILE)
        def _(n):
            c = pl.ds(pl.multiple_of(n * TILE, TILE), TILE)
            x = scaled[lines, :]
            norm = jnp.concatenate([squares[lines, :], squares[lines, :]], axis=1)
            gate = (gate_acc[lines, c] + dot(x, wg[start:start + CHUNK, c])) * norm
            upper = (up_acc[lines, c] + dot(x, wu[start:start + CHUNK, c])) * norm
            hid[:, c] = (gate / (1.0 + jnp.exp(-gate)) * upper).astype(jnp.bfloat16)

        @pl.loop(0, WIDTH // 512)
        def _(n):
            c = pl.ds(pl.multiple_of(n * 512, 512), 512)
            result = dot(hid[...], wd[:, c]).astype(jnp.bfloat16)
            ys[mine, :, c] = result.reshape(PER_GROUP, CAP, 512)

        for i in range(g * PER_GROUP, (g + 1) * PER_GROUP):
            if i == OWN:
                yr[i] = ys[i]
            else:
                a, b = SHIFTS[i]
                remote(ys.at[i], yr.at[i], y_send, y_recv.at[g], at(-a, -b))

    for g in range(GROUPS):
        wait_for(yr.at[pl.ds(g * PER_GROUP, remote_count(g))], y_recv.at[g])

        @pl.loop(0, WIDTH // 512)
        def _(n):
            c = pl.ds(pl.multiple_of(n * 512, 512), 512)
            lanes = slice(g * GROUP_ROWS, (g + 1) * GROUP_ROWS)
            got = yr[g * PER_GROUP:(g + 1) * PER_GROUP, :, c].reshape(GROUP_ROWS, 512)
            total = acc[:, c] + dot(mix_hi[:, lanes], got) + dot(mix_lo[:, lanes], got)
            if g < GROUPS - 1:
                acc[:, c] = total
            else:
                out_ref[0, :, c] = total.astype(jnp.bfloat16)

    for t, (src, dst) in enumerate(heads):
        wait_for(dst.at[pl.ds(0, ROWS * (N_SP - 1))], head_send.at[t])
    for i in range(2):
        wait_for(proj_a.at[three, half_rows], proj_send.at[i])
        wait_for(proj_a.at[three, half_rows], relay_send.at[i])
        wait_for(o_buf.at[three], o_send.at[i])
        wait_for(part_a.at[:, three], r_send.at[i])
    wait_for(xs.at[:, fifteen], d_send)
    wait_for(ys.at[fifteen], y_send)


def body(
    queries, keys, values, proj_weight, residual, norm_gain, route, route_weight,
    w_gate, w_up, w_down,
):
    bf16, f32 = jnp.bfloat16, jnp.float32
    vmem = pltpu.VMEM
    dma = pltpu.SemaphoreType.DMA
    anywhere = pl.BlockSpec(memory_space=pl.ANY)
    inside = pl.BlockSpec(memory_space=pltpu.VMEM)
    scratch = [
        vmem((LENGTH, HEAD), bf16), vmem((LENGTH, HEAD), bf16), vmem((LENGTH, HEAD), bf16),
        vmem((LENGTH, LENGTH), bf16), vmem((LENGTH, HEAD), f32), vmem((TILE, TILE + HEAD), bf16),
        vmem((SIDE, SIDE, ROWS, HEAD), bf16),
        vmem((SIDE, ROWS, 512), bf16), vmem((SIDE, ROWS, 512), bf16),
        vmem((SIDE, ROWS, HALF), bf16), vmem((SIDE, ROWS, HALF), bf16),
        vmem((2, SIDE, ROWS, CHUNK), bf16), vmem((2, SIDE, ROWS, CHUNK), bf16),
        vmem((2, SIDE, ROWS, CHUNK), bf16), vmem((2, SIDE, ROWS, CHUNK), bf16),
        vmem((ROWS, WIDTH), bf16), vmem((ROWS, WIDTH), f32),
        vmem((N_SP * CAP, ROWS), bf16), vmem((ROWS, N_SP * CAP), bf16), vmem((ROWS, N_SP * CAP), bf16),
        vmem((CHUNKS, N_SP, CAP, CHUNK), bf16), vmem((CHUNKS, N_SP, CAP, CHUNK), bf16),
        vmem((N_SP, CAP, WIDTH), bf16), vmem((N_SP, CAP, WIDTH), bf16),
        vmem((N_SP * CAP, CHUNK), bf16), vmem((N_SP * CAP, HEAD), f32),
        vmem((N_SP * CAP, FFE), f32), vmem((N_SP * CAP, FFE), f32),
        vmem((GROUP_ROWS, FFE), bf16),
        vmem((WIDTH, FFE), bf16), vmem((WIDTH, FFE), bf16), vmem((FFE, WIDTH), bf16),
        dma((6,)), dma((3,)), dma((3,)), dma((2,)), dma((2,)), dma((2,)), dma((2,)),
        dma((2,)), dma((SIDE,)), dma, dma((2,)), dma((2,)), dma((2,)),
        dma, dma((CHUNKS - 1 + GROUPS,)), dma, dma((GROUPS,)),
    ]
    return pl.pallas_call(
        body_kernel,
        out_shape=jax.ShapeDtypeStruct((1, ROWS, WIDTH), bf16),
        in_specs=[anywhere] * 5 + [inside] * 3 + [anywhere] * 3,
        out_specs=inside,
        scratch_shapes=scratch,
        compiler_params=pltpu.CompilerParams(
            collective_id=0, has_side_effects=True, vmem_limit_bytes=56 * 1024 * 1024
        ),
        name="layer",
    )(
        queries, keys, values, proj_weight, residual, norm_gain.reshape(1, WIDTH),
        jnp.swapaxes(route, 1, 2), jnp.swapaxes(route_weight, 1, 2), w_gate, w_up, w_down,
    )


def solution(mesh):
    return jax.shard_map(
        body,
        mesh=mesh,
        in_specs=(
            P("dp", "sp", None),
            P("dp", "sp", None),
            P("dp", "sp", None),
            P("sp", None),
            P("dp", "sp", None),
            P(),
            P("dp", "sp", None),
            P("dp", "sp", None),
            P("sp", None, None),
            P("sp", None, None),
            P("sp", None, None),
        ),
        out_specs=P("dp", "sp", None),
        check_vma=False,
    )
```

```python
import functools
import math

import jax
import jax.numpy as jnp
from jax import lax
from jax.experimental import pallas as pl
from jax.experimental.pallas import tpu as pltpu
from jax.sharding import PartitionSpec as P

MESH = pl.DeviceIdType.MESH
EPS = 1e-06
SIDE = 4
N_SP = 16
ROWS = 128
HEAD = 128
LENGTH = 2048
WIDTH = 2048
FFE = 1024
HALF = 1024
CHUNK = 512
CHUNKS = 4
CAP = 32
TILE = 256
LOG2E = 1.0 / math.log(2.0)

SHIFTS = (
    (1, 2), (3, 2), (2, 1), (2, 3),
    (2, 2), (2, 0), (0, 2), (0, 0),
    (1, 1), (3, 3), (1, 3), (3, 1),
    (1, 0), (3, 0), (0, 1), (0, 3),
)
OWN = SHIFTS.index((0, 0))
GROUPS = 4
PER_GROUP = 4
GROUP_ROWS = PER_GROUP * CAP


def dot(a, b):
    return jnp.dot(a, b, preferred_element_type=jnp.float32)


def body_kernel(
    q_hbm, k_hbm, v_hbm, proj_hbm, res_hbm, gain_ref, route_ref, rw_ref,
    wg_hbm, wu_hbm, wd_hbm,
    out_ref,
    qh, kh, vh, w_att, carry, tri, o_buf, oa, ob, proj_a, proj_b,
    part_a, part_b, sum_a, sum_b, res, acc, pick, mix_hi, mix_lo,
    xs, xr, ys, yr, scaled, squares, gate_acc, up_acc, hid, wg, wu, wd,
    local_sem, head_send, head_recv, proj_send, proj_recv, relay_send, relay_recv,
    o_send, oa_recv, ob_recv, r_send, ra_recv, rb_recv, d_send, d_recv, y_send, y_recv,
):
    me = lax.axis_index("sp")
    dp = lax.axis_index("dp")
    z = me // SIDE
    y = me % SIDE
    core = dp % 2
    partner = dp + 1 - 2 * core

    def at(a, b):
        return ((z + a) % SIDE) * SIDE + (y + b) % SIDE

    others = [s for s in SHIFTS if s != (0, 0)]
    line = (2, 1, 3)

    barrier = pltpu.get_barrier_semaphore()
    for a, b in others:
        pl.semaphore_signal(barrier, inc=1, device_id={"sp": at(a, b)}, device_id_type=MESH)
    pl.semaphore_signal(barrier, inc=1, device_id={"dp": partner}, device_id_type=MESH)

    def local(src, dst, sem):
        copy = pltpu.make_async_copy(src, dst, sem)
        copy.start()
        return copy

    def remote(src, dst, send, recv, peer, axis="sp"):
        pltpu.make_async_remote_copy(
            src_ref=src, dst_ref=dst, send_sem=send, recv_sem=recv,
            device_id={axis: peer}, device_id_type=MESH,
        ).start()

    def wait_for(ref, sem):
        pltpu.make_async_copy(ref, ref, sem).wait()

    my_rows = pl.ds(pl.multiple_of(me * ROWS, ROWS), ROWS)
    core_rows = pl.ds(pl.multiple_of(core * (ROWS // 2), ROWS // 2), ROWS // 2)

    def cols(peer):
        return pl.ds(pl.multiple_of(peer * HEAD, HEAD), HEAD)

    heads = ((k_hbm, kh), (q_hbm, qh), (v_hbm, vh))
    for t, (src, dst) in enumerate(heads):
        local(src.at[0, :, cols(me)], dst.at[my_rows], head_recv.at[t])
    loads = [
        local(proj_hbm.at[:, pl.ds(0, HALF)], proj_a.at[y], local_sem.at[4]),
        local(proj_hbm.at[:, pl.ds(HALF, HALF)], proj_b.at[z], local_sem.at[5]),
    ]

    pl.semaphore_wait(barrier, N_SP)

    def send_heads(t, a, b):
        src, dst = heads[t]
        peer = at(a, b)
        remote(src.at[0, :, cols(peer)], dst.at[my_rows], head_send.at[t], head_recv.at[t], peer)

    for a, b in others:
        send_heads(0, a, b)
        send_heads(1, a, b)
    for a, b in others:
        send_heads(2, a, b)
    for s in line:
        remote(proj_hbm.at[core_rows, pl.ds(0, HALF)], proj_a.at[y, core_rows],
               proj_send.at[0], proj_recv.at[0], at(0, s))
    for s in line:
        remote(proj_hbm.at[core_rows, pl.ds(HALF, HALF)], proj_b.at[z, core_rows],
               proj_send.at[1], proj_recv.at[1], at(s, 0))
    loads += [
        local(res_hbm.at[0], res, local_sem.at[0]),
        local(wg_hbm.at[0], wg, local_sem.at[1]),
        local(wu_hbm.at[0], wu, local_sem.at[2]),
        local(wd_hbm.at[0], wd, local_sem.at[3]),
    ]

    j = lax.broadcasted_iota(jnp.int32, (TILE, TILE + HEAD), 0)
    s = lax.broadcasted_iota(jnp.int32, (TILE, TILE + HEAD), 1)
    tri[...] = jnp.where((j > s) | (s >= TILE), 1.0, 0.0).astype(jnp.bfloat16)

    @pl.loop(0, LENGTH // 64)
    def _(i):
        w_att[pl.ds(pl.multiple_of(i * 64, 64), 64), :] = jnp.zeros((64, LENGTH), jnp.bfloat16)

    slots = N_SP * CAP
    lane = lax.broadcasted_iota(jnp.int32, (ROWS, slots), 1)
    place = lane // CAP
    expert = jnp.zeros((ROWS, slots), jnp.int32)
    for i, (a, b) in enumerate(SHIFTS):
        expert = jnp.where(place == i, at(a, b), expert)
    zeros = jnp.zeros((6, ROWS), jnp.float32)
    route = jnp.concatenate([route_ref[0].astype(jnp.float32), zeros], axis=0).T
    share = jnp.concatenate([rw_ref[0], zeros], axis=0).T
    expert = expert.astype(jnp.float32)
    first = route[:, 0:1] == expert
    second = route[:, 1:2] == expert
    named = jnp.where(first | second, 1.0, 0.0)
    r0 = lax.broadcasted_iota(jnp.int32, (ROWS, ROWS), 0)
    r1 = lax.broadcasted_iota(jnp.int32, (ROWS, ROWS), 1)
    before = jnp.where(r1 < r0, 1.0, 0.0).astype(jnp.bfloat16)
    slot = dot(before, named.astype(jnp.bfloat16))
    held = jnp.where(slot == (lane - place * CAP).astype(jnp.float32), named, 0.0)
    pick[...] = held.T.astype(jnp.bfloat16)
    mix = held * jnp.where(first, share[:, 0:1], share[:, 1:2])
    high = mix.astype(jnp.bfloat16)
    mix_hi[...] = high
    mix_lo[...] = (mix - high.astype(jnp.float32)).astype(jnp.bfloat16)

    wait_for(kh, head_recv.at[0])
    wait_for(qh, head_recv.at[1])
    scale = HEAD ** (-0.5) * LOG2E

    def weights(q0, k0, diagonal):
        q_rows = pl.ds(q0, TILE)
        k_rows = pl.ds(k0, TILE)
        u = lax.dot_general(
            qh[q_rows, :], kh[k_rows, :], (((1,), (1,)), ((), ())),
            preferred_element_type=jnp.float32,
        ) * scale
        low = jnp.log(1.0 + jnp.exp2(-jnp.abs(u))) * LOG2E
        soft = jnp.maximum(u, 0.0) + low
        if diagonal:
            causal = lax.broadcasted_iota(jnp.int32, (TILE, TILE), 1) < lax.broadcasted_iota(
                jnp.int32, (TILE, TILE), 0
            )
            soft = jnp.where(causal, soft, 0.0)
        sums = dot(soft.astype(jnp.bfloat16), tri[...])
        power = jnp.minimum(u, 0.0) - low - sums[:, :TILE]
        total = sums[:, TILE:]
        if not diagonal:
            later = carry[q_rows, :]
            power = power - jnp.concatenate([later, later], axis=1)
            total = total + later
        weight = jnp.exp2(power)
        if diagonal:
            weight = jnp.where(causal, weight, 0.0)
        w_att[q_rows, k_rows] = weight.astype(jnp.bfloat16)
        carry[q_rows, :] = total

    def quarter_weights(quarter):
        base = pl.multiple_of(quarter * 512, 512)
        weights(pl.multiple_of(base + TILE, TILE), pl.multiple_of(base + TILE, TILE), True)
        weights(base, base, True)
        weights(pl.multiple_of(base + TILE, TILE), base, False)

        @pl.loop(0, 2 * quarter)
        def _(i):
            k0 = pl.multiple_of((2 * quarter - 1 - i) * TILE, TILE)
            for half in range(2):
                weights(pl.multiple_of(base + half * TILE, TILE), k0, False)

    def quarter_values(i):
        quarter = (z + 1 + i) % SIDE
        rows = pl.ds(pl.multiple_of(quarter * 512, 512), 512)
        o_buf[quarter] = dot(w_att[rows, :], vh[...]).astype(jnp.bfloat16).reshape(SIDE, ROWS, HEAD)
        if i < SIDE - 1:
            remote(o_buf.at[quarter], ob.at[:, :, cols(z)], o_send.at[1], ob_recv, quarter * SIDE + y)
        else:
            ob[:, :, cols(z)] = o_buf[z]
        for s in line:
            peer_y = (y + s) % SIDE
            remote(o_buf.at[quarter, peer_y], oa.at[quarter, :, cols(y)], o_send.at[0],
                   oa_recv.at[quarter], z * SIDE + peer_y)
        oa[quarter, :, cols(y)] = o_buf[quarter, y]

    quarter_weights((z + 1) % SIDE)
    quarter_weights((z + 2) % SIDE)
    wait_for(vh, head_recv.at[2])
    quarter_values(0)
    quarter_values(1)
    quarter_weights((z + 3) % SIDE)
    quarter_values(2)
    quarter_weights(z)
    quarter_values(3)

    three = pl.ds(0, SIDE - 1)
    half_rows = pl.ds(0, ROWS // 2)
    for index, (weight, mine) in enumerate(((proj_a, y), (proj_b, z))):
        wait_for(weight.at[three, half_rows], proj_recv.at[index])
        for s in line:
            piece = weight.at[(mine + s) % SIDE, core_rows]
            remote(piece, piece, relay_send.at[index], relay_recv.at[index], partner, "dp")

    loads[0].wait()
    wait_for(proj_a.at[three, half_rows], relay_recv.at[0])
    for i in range(SIDE):
        quarter = (z + 1 + i) % SIDE
        wait_for(oa.at[0, :, pl.ds(0, 3 * HEAD)], oa_recv.at[quarter])
        left = oa[quarter]
        for q in range(2):
            for n in range(2):
                c = slice(q * CHUNK + n * TILE, q * CHUNK + (n + 1) * TILE)
                right = proj_a[:, :, c].reshape(512, TILE)
                part_a[q, quarter, :, n * TILE:(n + 1) * TILE] = dot(left, right).astype(jnp.bfloat16)
        if i < SIDE - 1:
            remote(part_a.at[0, quarter], sum_a.at[0, z], r_send.at[0], ra_recv.at[0], quarter * SIDE + y)
    for s in (1, 2, 3):
        peer_z = (z + s) % SIDE
        remote(part_a.at[1, peer_z], sum_a.at[1, z], r_send.at[0], ra_recv.at[1], peer_z * SIDE + y)
    loads[1].wait()
    wait_for(proj_b.at[three, half_rows], relay_recv.at[1])
    wait_for(ob.at[:, :, pl.ds(0, 3 * HEAD)], ob_recv)
    for q in range(2):
        @pl.loop(0, 2)
        def _(n):
            c = pl.ds(pl.multiple_of(q * CHUNK + n * TILE, TILE), TILE)
            right = proj_b[:, :, c].reshape(512, TILE)
            block = dot(ob[...].reshape(512, 512), right).astype(jnp.bfloat16)
            part_b[q, :, :, pl.ds(pl.multiple_of(n * TILE, TILE), TILE)] = block.reshape(SIDE, ROWS, TILE)

        for s in line:
            peer_y = (y + s) % SIDE
            remote(part_b.at[q, peer_y], sum_b.at[q, y], r_send.at[1], rb_recv.at[q], z * SIDE + peer_y)
    for q in range(2):
        sum_a[q, z] = part_a[q, z]
        sum_b[q, y] = part_b[q, y]

    pieces = ((sum_a, ra_recv, 0, 0), (sum_b, rb_recv, 0, HALF),
              (sum_a, ra_recv, 1, CHUNK), (sum_b, rb_recv, 1, HALF + CHUNK))
    loads[2].wait()
    for k, (sums, recv, q, start) in enumerate(pieces):
        wait_for(sums.at[q, three], recv.at[q])
        total = res[:, start:start + CHUNK].astype(jnp.float32)
        for i in range(SIDE):
            total = total + sums[q, i].astype(jnp.float32)
        stream = total.astype(jnp.bfloat16)
        acc[:, start:start + CHUNK] = stream.astype(jnp.float32)
        for n in range(2):
            c = slice(n * TILE, (n + 1) * TILE)
            rows = dot(pick[...], stream[:, c]).astype(jnp.bfloat16)
            xs[k, :, :, c] = rows.reshape(N_SP, CAP, TILE)
        for i, (a, b) in enumerate(SHIFTS):
            if i != OWN:
                sem = d_recv.at[k] if k < CHUNKS - 1 else d_recv.at[k + i // PER_GROUP]
                remote(xs.at[k, i], xr.at[k, i], d_send, sem, at(a, b))
        xr[k, OWN] = xs[k, OWN]

    for load in loads[3:]:
        load.wait()
    fifteen = pl.ds(0, N_SP - 1)
    for k in range(CHUNKS - 1):
        start = pieces[k][3]
        wait_for(xr.at[k, fifteen], d_recv.at[k])

        @pl.loop(0, N_SP // 2)
        def _(i):
            rows = xr[k, pl.ds(2 * i, 2)].astype(jnp.float32).reshape(2 * CAP, CHUNK)
            r = pl.ds(pl.multiple_of(i * 2 * CAP, 2 * CAP), 2 * CAP)
            scaled[r, :] = (rows * gain_ref[:, start:start + CHUNK]).astype(jnp.bfloat16)
            square = jnp.sum(rows * rows, axis=-1, keepdims=True)
            square = jnp.broadcast_to(square, (2 * CAP, HEAD))
            squares[r, :] = square if k == 0 else squares[r, :] + square

        @pl.loop(0, FFE // TILE)
        def _(n):
            c = pl.ds(pl.multiple_of(n * TILE, TILE), TILE)
            for weight, total in ((wg, gate_acc), (wu, up_acc)):
                new = dot(scaled[...], weight[start:start + CHUNK, c])
                total[:, c] = new if k == 0 else total[:, c] + new

    def remote_count(g):
        return PER_GROUP - (1 if OWN // PER_GROUP == g else 0)

    last = CHUNKS - 1
    start = pieces[last][3]
    for g in range(GROUPS):
        mine = slice(g * PER_GROUP, (g + 1) * PER_GROUP)
        lines = slice(g * GROUP_ROWS, (g + 1) * GROUP_ROWS)
        wait_for(xr.at[last, pl.ds(g * PER_GROUP, remote_count(g))], d_recv.at[last + g])
        rows = xr[last, mine].astype(jnp.float32).reshape(GROUP_ROWS, CHUNK)
        scaled[lines, :] = (rows * gain_ref[:, start:start + CHUNK]).astype(jnp.bfloat16)
        square = squares[lines, 0:1] + jnp.sum(rows * rows, axis=-1, keepdims=True)
        factor = lax.rsqrt(square * (1.0 / WIDTH) + EPS)

        norm = jnp.broadcast_to(factor, (GROUP_ROWS, TILE))
        for n in range(FFE // TILE):
            c = slice(n * TILE, (n + 1) * TILE)
            x = scaled[lines, :]
            gate = (gate_acc[lines, c] + dot(x, wg[start:start + CHUNK, c])) * norm
            upper = (up_acc[lines, c] + dot(x, wu[start:start + CHUNK, c])) * norm
            hid[:, c] = (gate / (1.0 + jnp.exp(-gate)) * upper).astype(jnp.bfloat16)

        for n in range(WIDTH // TILE):
            c = slice(n * TILE, (n + 1) * TILE)
            result = dot(hid[...], wd[:, c]).astype(jnp.bfloat16)
            ys[mine, :, c] = result.reshape(PER_GROUP, CAP, TILE)

        for i in range(g * PER_GROUP, (g + 1) * PER_GROUP):
            if i == OWN:
                yr[i] = ys[i]
            else:
                a, b = SHIFTS[i]
                remote(ys.at[i], yr.at[i], y_send, y_recv.at[g], at(-a, -b))

    for g in range(GROUPS):
        wait_for(yr.at[pl.ds(g * PER_GROUP, remote_count(g))], y_recv.at[g])

        for n in range(WIDTH // 512):
            c = slice(n * 512, (n + 1) * 512)
            lanes = slice(g * GROUP_ROWS, (g + 1) * GROUP_ROWS)
            got = yr[g * PER_GROUP:(g + 1) * PER_GROUP, :, c].reshape(GROUP_ROWS, 512)
            total = acc[:, c] + dot(mix_hi[:, lanes], got) + dot(mix_lo[:, lanes], got)
            if g < GROUPS - 1:
                acc[:, c] = total
            else:
                out_ref[0, :, c] = total.astype(jnp.bfloat16)

    for t, (src, dst) in enumerate(heads):
        wait_for(dst.at[pl.ds(0, ROWS * (N_SP - 1))], head_send.at[t])
    for i in range(2):
        wait_for(proj_a.at[three, half_rows], proj_send.at[i])
        wait_for(proj_a.at[three, half_rows], relay_send.at[i])
        wait_for(o_buf.at[three], o_send.at[i])
        wait_for(part_a.at[:, three], r_send.at[i])
    wait_for(xs.at[:, fifteen], d_send)
    wait_for(ys.at[fifteen], y_send)


def body(
    queries, keys, values, proj_weight, residual, norm_gain, route, route_weight,
    w_gate, w_up, w_down,
):
    bf16, f32 = jnp.bfloat16, jnp.float32
    vmem = pltpu.VMEM
    dma = pltpu.SemaphoreType.DMA
    anywhere = pl.BlockSpec(memory_space=pl.ANY)
    inside = pl.BlockSpec(memory_space=pltpu.VMEM)
    scratch = [
        vmem((LENGTH, HEAD), bf16), vmem((LENGTH, HEAD), bf16), vmem((LENGTH, HEAD), bf16),
        vmem((LENGTH, LENGTH), bf16), vmem((LENGTH, HEAD), f32), vmem((TILE, TILE + HEAD), bf16),
        vmem((SIDE, SIDE, ROWS, HEAD), bf16),
        vmem((SIDE, ROWS, 512), bf16), vmem((SIDE, ROWS, 512), bf16),
        vmem((SIDE, ROWS, HALF), bf16), vmem((SIDE, ROWS, HALF), bf16),
        vmem((2, SIDE, ROWS, CHUNK), bf16), vmem((2, SIDE, ROWS, CHUNK), bf16),
        vmem((2, SIDE, ROWS, CHUNK), bf16), vmem((2, SIDE, ROWS, CHUNK), bf16),
        vmem((ROWS, WIDTH), bf16), vmem((ROWS, WIDTH), f32),
        vmem((N_SP * CAP, ROWS), bf16), vmem((ROWS, N_SP * CAP), bf16), vmem((ROWS, N_SP * CAP), bf16),
        vmem((CHUNKS, N_SP, CAP, CHUNK), bf16), vmem((CHUNKS, N_SP, CAP, CHUNK), bf16),
        vmem((N_SP, CAP, WIDTH), bf16), vmem((N_SP, CAP, WIDTH), bf16),
        vmem((N_SP * CAP, CHUNK), bf16), vmem((N_SP * CAP, HEAD), f32),
        vmem((N_SP * CAP, FFE), f32), vmem((N_SP * CAP, FFE), f32),
        vmem((GROUP_ROWS, FFE), bf16),
        vmem((WIDTH, FFE), bf16), vmem((WIDTH, FFE), bf16), vmem((FFE, WIDTH), bf16),
        dma((6,)), dma((3,)), dma((3,)), dma((2,)), dma((2,)), dma((2,)), dma((2,)),
        dma((2,)), dma((SIDE,)), dma, dma((2,)), dma((2,)), dma((2,)),
        dma, dma((CHUNKS - 1 + GROUPS,)), dma, dma((GROUPS,)),
    ]
    return pl.pallas_call(
        body_kernel,
        out_shape=jax.ShapeDtypeStruct((1, ROWS, WIDTH), bf16),
        in_specs=[anywhere] * 5 + [inside] * 3 + [anywhere] * 3,
        out_specs=inside,
        scratch_shapes=scratch,
        compiler_params=pltpu.CompilerParams(
            collective_id=0, has_side_effects=True, vmem_limit_bytes=56 * 1024 * 1024
        ),
        name="layer",
    )(
        queries, keys, values, proj_weight, residual, norm_gain.reshape(1, WIDTH),
        jnp.swapaxes(route, 1, 2), jnp.swapaxes(route_weight, 1, 2), w_gate, w_up, w_down,
    )


def solution(mesh):
    return jax.shard_map(
        body,
        mesh=mesh,
        in_specs=(
            P("dp", "sp", None),
            P("dp", "sp", None),
            P("dp", "sp", None),
            P("sp", None),
            P("dp", "sp", None),
            P(),
            P("dp", "sp", None),
            P("dp", "sp", None),
            P("sp", None, None),
            P("sp", None, None),
            P("sp", None, None),
        ),
        out_specs=P("dp", "sp", None),
        check_vma=False,
    )
```

```python
import functools
import math

import jax
import jax.numpy as jnp
from jax import lax
from jax.experimental import pallas as pl
from jax.experimental.pallas import tpu as pltpu
from jax.sharding import PartitionSpec as P

MESH = pl.DeviceIdType.MESH
EPS = 1e-06
SIDE = 4
N_SP = 16
ROWS = 128
HEAD = 128
LENGTH = 2048
WIDTH = 2048
FFE = 1024
HALF = 1024
CHUNK = 512
CHUNKS = 4
CAP = 32
TILE = 256
LOG2E = 1.0 / math.log(2.0)

SHIFTS = (
    (1, 2), (3, 2), (2, 1), (2, 3),
    (2, 2), (2, 0), (0, 2), (0, 0),
    (1, 1), (3, 3), (1, 3), (3, 1),
    (1, 0), (3, 0), (0, 1), (0, 3),
)
OWN = SHIFTS.index((0, 0))
GROUPS = 4
PER_GROUP = 4
GROUP_ROWS = PER_GROUP * CAP


def dot(a, b):
    return jnp.dot(a, b, preferred_element_type=jnp.float32)


def body_kernel(
    q_hbm, k_hbm, v_hbm, proj_hbm, res_hbm, gain_ref, route_ref, rw_ref,
    wg_hbm, wu_hbm, wd_hbm,
    out_ref,
    qh, kh, vh, w_att, carry, softer, power, tri, o_buf, oa, ob, proj_a, proj_b,
    part_a, part_b, sum_a, sum_b, res, acc, pick, mix_hi, mix_lo,
    xs, xr, ys, yr, scaled, squares, gate_acc, up_acc, hid, wg, wu, wd,
    local_sem, head_send, head_recv, proj_send, proj_recv, relay_send, relay_recv,
    o_send, oa_recv, ob_recv, r_send, ra_recv, rb_recv, d_send, d_recv, y_send, y_recv,
):
    me = lax.axis_index("sp")
    dp = lax.axis_index("dp")
    z = me // SIDE
    y = me % SIDE
    core = dp % 2
    partner = dp + 1 - 2 * core

    def at(a, b):
        return ((z + a) % SIDE) * SIDE + (y + b) % SIDE

    others = [s for s in SHIFTS if s != (0, 0)]
    line = (2, 1, 3)

    barrier = pltpu.get_barrier_semaphore()
    for a, b in others:
        pl.semaphore_signal(barrier, inc=1, device_id={"sp": at(a, b)}, device_id_type=MESH)
    pl.semaphore_signal(barrier, inc=1, device_id={"dp": partner}, device_id_type=MESH)

    def local(src, dst, sem):
        copy = pltpu.make_async_copy(src, dst, sem)
        copy.start()
        return copy

    def remote(src, dst, send, recv, peer, axis="sp"):
        pltpu.make_async_remote_copy(
            src_ref=src, dst_ref=dst, send_sem=send, recv_sem=recv,
            device_id={axis: peer}, device_id_type=MESH,
        ).start()

    def wait_for(ref, sem):
        pltpu.make_async_copy(ref, ref, sem).wait()

    my_rows = pl.ds(pl.multiple_of(me * ROWS, ROWS), ROWS)
    core_rows = pl.ds(pl.multiple_of(core * (ROWS // 2), ROWS // 2), ROWS // 2)

    def cols(peer):
        return pl.ds(pl.multiple_of(peer * HEAD, HEAD), HEAD)

    heads = ((k_hbm, kh), (q_hbm, qh), (v_hbm, vh))
    for t, (src, dst) in enumerate(heads):
        local(src.at[0, :, cols(me)], dst.at[my_rows], head_recv.at[t])
    loads = [
        local(proj_hbm.at[:, pl.ds(0, HALF)], proj_a.at[y], local_sem.at[4]),
        local(proj_hbm.at[:, pl.ds(HALF, HALF)], proj_b.at[z], local_sem.at[5]),
    ]

    pl.semaphore_wait(barrier, N_SP)

    def send_heads(t, a, b):
        src, dst = heads[t]
        peer = at(a, b)
        remote(src.at[0, :, cols(peer)], dst.at[my_rows], head_send.at[t], head_recv.at[t], peer)

    for a, b in others:
        send_heads(0, a, b)
        send_heads(1, a, b)
    for a, b in others:
        send_heads(2, a, b)
    for s in line:
        remote(proj_hbm.at[core_rows, pl.ds(0, HALF)], proj_a.at[y, core_rows],
               proj_send.at[0], proj_recv.at[0], at(0, s))
    for s in line:
        remote(proj_hbm.at[core_rows, pl.ds(HALF, HALF)], proj_b.at[z, core_rows],
               proj_send.at[1], proj_recv.at[1], at(s, 0))
    loads += [
        local(res_hbm.at[0], res, local_sem.at[0]),
        local(wg_hbm.at[0], wg, local_sem.at[1]),
        local(wu_hbm.at[0], wu, local_sem.at[2]),
        local(wd_hbm.at[0], wd, local_sem.at[3]),
    ]

    j = lax.broadcasted_iota(jnp.int32, (TILE, TILE + HEAD), 0)
    s = lax.broadcasted_iota(jnp.int32, (TILE, TILE + HEAD), 1)
    tri[...] = jnp.where((j > s) | (s >= TILE), 1.0, 0.0).astype(jnp.bfloat16)

    @pl.loop(0, LENGTH // 64)
    def _(i):
        w_att[pl.ds(pl.multiple_of(i * 64, 64), 64), :] = jnp.zeros((64, LENGTH), jnp.bfloat16)

    slots = N_SP * CAP
    lane = lax.broadcasted_iota(jnp.int32, (ROWS, slots), 1)
    place = lane // CAP
    expert = jnp.zeros((ROWS, slots), jnp.int32)
    for i, (a, b) in enumerate(SHIFTS):
        expert = jnp.where(place == i, at(a, b), expert)
    zeros = jnp.zeros((6, ROWS), jnp.float32)
    route = jnp.concatenate([route_ref[0].astype(jnp.float32), zeros], axis=0).T
    share = jnp.concatenate([rw_ref[0], zeros], axis=0).T
    expert = expert.astype(jnp.float32)
    first = route[:, 0:1] == expert
    second = route[:, 1:2] == expert
    named = jnp.where(first | second, 1.0, 0.0)
    r0 = lax.broadcasted_iota(jnp.int32, (ROWS, ROWS), 0)
    r1 = lax.broadcasted_iota(jnp.int32, (ROWS, ROWS), 1)
    before = jnp.where(r1 < r0, 1.0, 0.0).astype(jnp.bfloat16)
    slot = dot(before, named.astype(jnp.bfloat16))
    held = jnp.where(slot == (lane - place * CAP).astype(jnp.float32), named, 0.0)
    pick[...] = held.T.astype(jnp.bfloat16)
    mix = held * jnp.where(first, share[:, 0:1], share[:, 1:2])
    high = mix.astype(jnp.bfloat16)
    mix_hi[...] = high
    mix_lo[...] = (mix - high.astype(jnp.float32)).astype(jnp.bfloat16)

    wait_for(kh, head_recv.at[0])
    wait_for(qh, head_recv.at[1])
    scale = HEAD ** (-0.5)

    causal = lax.broadcasted_iota(jnp.int32, (TILE, TILE), 1) < lax.broadcasted_iota(
        jnp.int32, (TILE, TILE), 0
    )

    def soften(base, lines, k0, which, diagonal):
        rows = slice(*lines)
        u = lax.dot_general(
            qh[pl.ds(pl.multiple_of(base + lines[0], TILE), lines[1] - lines[0]), :],
            kh[pl.ds(k0, TILE), :], (((1,), (1,)), ((), ())),
            preferred_element_type=jnp.float32,
        ) * scale
        low = jnp.log(1.0 + jnp.exp2(jnp.abs(u) * -LOG2E))
        soft = jnp.maximum(u, 0.0) + low
        if diagonal:
            soft = jnp.where(causal, soft, 0.0)
        softer[which, rows, :] = soft.astype(jnp.bfloat16)
        power[which, rows, :] = jnp.minimum(u, 0.0) - low

    def weigh(base, lines, k0, which, diagonal, fresh):
        rows = slice(*lines)
        sums = dot(softer[which, rows, :], tri[...])
        less = sums[:, :TILE]
        total = sums[:, TILE:]
        if not fresh:
            later = carry[rows, :]
            less = less + jnp.concatenate([later, later], axis=1)
            total = total + later
        weight = jnp.exp2((power[which, rows, :] - less) * LOG2E)
        if diagonal:
            weight = jnp.where(causal, weight, 0.0)
        place = pl.ds(pl.multiple_of(base + lines[0], TILE), lines[1] - lines[0])
        w_att[place, pl.ds(k0, TILE)] = weight.astype(jnp.bfloat16)
        carry[rows, :] = total

    upper, lower, both = (0, TILE), (TILE, 2 * TILE), (0, 2 * TILE)

    def quarter_weights(quarter):
        base = pl.multiple_of(quarter * 512, 512)
        second = pl.multiple_of(base + TILE, TILE)
        soften(base, lower, second, 1, True)
        soften(base, upper, base, 0, True)
        soften(base, lower, base, 0, False)
        weigh(base, lower, second, 1, True, True)
        weigh(base, upper, base, 0, True, True)
        weigh(base, lower, base, 0, False, False)

        @pl.loop(0, quarter)
        def _(i):
            for which in range(2):
                k0 = pl.multiple_of((2 * quarter - 2 * i - 1 - which) * TILE, TILE)
                soften(base, both, k0, which, False)
                weigh(base, both, k0, which, False, False)

    def quarter_values(i):
        quarter = (z + 1 + i) % SIDE
        rows = pl.ds(pl.multiple_of(quarter * 512, 512), 512)
        o_buf[quarter] = dot(w_att[rows, :], vh[...]).astype(jnp.bfloat16).reshape(SIDE, ROWS, HEAD)
        if i < SIDE - 1:
            remote(o_buf.at[quarter], ob.at[:, :, cols(z)], o_send.at[1], ob_recv, quarter * SIDE + y)
        else:
            ob[:, :, cols(z)] = o_buf[z]
        for s in line:
            peer_y = (y + s) % SIDE
            remote(o_buf.at[quarter, peer_y], oa.at[quarter, :, cols(y)], o_send.at[0],
                   oa_recv.at[quarter], z * SIDE + peer_y)
        oa[quarter, :, cols(y)] = o_buf[quarter, y]

    three = pl.ds(0, SIDE - 1)
    half_rows = pl.ds(0, ROWS // 2)

    def relay():
        for index, (weight, mine) in enumerate(((proj_a, y), (proj_b, z))):
            wait_for(weight.at[three, half_rows], proj_recv.at[index])
            for s in line:
                piece = weight.at[(mine + s) % SIDE, core_rows]
                remote(piece, piece, relay_send.at[index], relay_recv.at[index], partner, "dp")

    def project_z(i):
        quarter = (z + 1 + i) % SIDE
        wait_for(oa.at[0, :, pl.ds(0, 3 * HEAD)], oa_recv.at[quarter])
        left = oa[quarter]
        for q in range(2):
            for n in range(2):
                c = slice(q * CHUNK + n * TILE, q * CHUNK + (n + 1) * TILE)
                right = proj_a[:, :, c].reshape(512, TILE)
                part_a[q, quarter, :, n * TILE:(n + 1) * TILE] = dot(left, right).astype(jnp.bfloat16)
            if i < SIDE - 1:
                remote(part_a.at[q, quarter], sum_a.at[q, z], r_send.at[0], ra_recv.at[q], quarter * SIDE + y)

    def project_y(q):
        @pl.loop(0, 2)
        def _(n):
            c = pl.ds(pl.multiple_of(q * CHUNK + n * TILE, TILE), TILE)
            right = proj_b[:, :, c].reshape(512, TILE)
            block = dot(ob[...].reshape(512, 512), right).astype(jnp.bfloat16)
            part_b[q, :, :, pl.ds(pl.multiple_of(n * TILE, TILE), TILE)] = block.reshape(SIDE, ROWS, TILE)

        for s in line:
            peer_y = (y + s) % SIDE
            remote(part_b.at[q, peer_y], sum_b.at[q, y], r_send.at[1], rb_recv.at[q], z * SIDE + peer_y)

    quarter_weights((z + 1) % SIDE)
    quarter_weights((z + 2) % SIDE)
    wait_for(vh, head_recv.at[2])
    quarter_values(0)
    quarter_values(1)
    quarter_weights((z + 3) % SIDE)
    quarter_values(2)
    relay()
    loads[0].wait()
    loads[1].wait()
    wait_for(proj_a.at[three, half_rows], relay_recv.at[0])
    project_z(0)
    project_z(1)
    quarter_weights(z)
    quarter_values(3)
    wait_for(proj_b.at[three, half_rows], relay_recv.at[1])
    wait_for(ob.at[:, :, pl.ds(0, 3 * HEAD)], ob_recv)
    project_y(0)
    project_z(2)
    project_y(1)
    project_z(3)
    for q in range(2):
        sum_a[q, z] = part_a[q, z]
        sum_b[q, y] = part_b[q, y]

    pieces = ((sum_a, ra_recv, 0, 0), (sum_b, rb_recv, 0, HALF),
              (sum_a, ra_recv, 1, CHUNK), (sum_b, rb_recv, 1, HALF + CHUNK))
    loads[2].wait()
    for k, (sums, recv, q, start) in enumerate(pieces):
        wait_for(sums.at[q, three], recv.at[q])
        total = res[:, start:start + CHUNK].astype(jnp.float32)
        for i in range(SIDE):
            total = total + sums[q, i].astype(jnp.float32)
        stream = total.astype(jnp.bfloat16)
        acc[:, start:start + CHUNK] = stream.astype(jnp.float32)
        for n in range(2):
            c = slice(n * TILE, (n + 1) * TILE)
            rows = dot(pick[...], stream[:, c]).astype(jnp.bfloat16)
            xs[k, :, :, c] = rows.reshape(N_SP, CAP, TILE)
        for i, (a, b) in enumerate(SHIFTS):
            if i != OWN:
                sem = d_recv.at[k] if k < CHUNKS - 1 else d_recv.at[k + i // PER_GROUP]
                remote(xs.at[k, i], xr.at[k, i], d_send, sem, at(a, b))
        xr[k, OWN] = xs[k, OWN]

    for load in loads[3:]:
        load.wait()
    fifteen = pl.ds(0, N_SP - 1)
    for k in range(CHUNKS - 1):
        start = pieces[k][3]
        wait_for(xr.at[k, fifteen], d_recv.at[k])

        @pl.loop(0, N_SP // 2)
        def _(i):
            rows = xr[k, pl.ds(2 * i, 2)].astype(jnp.float32).reshape(2 * CAP, CHUNK)
            r = pl.ds(pl.multiple_of(i * 2 * CAP, 2 * CAP), 2 * CAP)
            scaled[r, :] = (rows * gain_ref[:, start:start + CHUNK]).astype(jnp.bfloat16)
            square = jnp.sum(rows * rows, axis=-1, keepdims=True)
            square = jnp.broadcast_to(square, (2 * CAP, HEAD))
            squares[r, :] = square if k == 0 else squares[r, :] + square

        @pl.loop(0, FFE // TILE)
        def _(n):
            c = pl.ds(pl.multiple_of(n * TILE, TILE), TILE)
            for weight, total in ((wg, gate_acc), (wu, up_acc)):
                new = dot(scaled[...], weight[start:start + CHUNK, c])
                total[:, c] = new if k == 0 else total[:, c] + new

    def remote_count(g):
        return PER_GROUP - (1 if OWN // PER_GROUP == g else 0)

    last = CHUNKS - 1
    start = pieces[last][3]
    for g in range(GROUPS):
        mine = slice(g * PER_GROUP, (g + 1) * PER_GROUP)
        lines = slice(g * GROUP_ROWS, (g + 1) * GROUP_ROWS)
        wait_for(xr.at[last, pl.ds(g * PER_GROUP, remote_count(g))], d_recv.at[last + g])
        rows = xr[last, mine].astype(jnp.float32).reshape(GROUP_ROWS, CHUNK)
        scaled[lines, :] = (rows * gain_ref[:, start:start + CHUNK]).astype(jnp.bfloat16)
        square = squares[lines, 0:1] + jnp.sum(rows * rows, axis=-1, keepdims=True)
        factor = lax.rsqrt(square * (1.0 / WIDTH) + EPS)

        norm = jnp.broadcast_to(factor, (GROUP_ROWS, TILE))
        for n in range(FFE // TILE):
            c = slice(n * TILE, (n + 1) * TILE)
            x = scaled[lines, :]
            gate = (gate_acc[lines, c] + dot(x, wg[start:start + CHUNK, c])) * norm
            upper = (up_acc[lines, c] + dot(x, wu[start:start + CHUNK, c])) * norm
            hid[:, c] = (gate / (1.0 + jnp.exp(-gate)) * upper).astype(jnp.bfloat16)

        for n in range(WIDTH // TILE):
            c = slice(n * TILE, (n + 1) * TILE)
            result = dot(hid[...], wd[:, c]).astype(jnp.bfloat16)
            ys[mine, :, c] = result.reshape(PER_GROUP, CAP, TILE)

        for i in range(g * PER_GROUP, (g + 1) * PER_GROUP):
            if i == OWN:
                yr[i] = ys[i]
            else:
                a, b = SHIFTS[i]
                remote(ys.at[i], yr.at[i], y_send, y_recv.at[g], at(-a, -b))

    for g in range(GROUPS):
        wait_for(yr.at[pl.ds(g * PER_GROUP, remote_count(g))], y_recv.at[g])

        for n in range(WIDTH // 512):
            c = slice(n * 512, (n + 1) * 512)
            lanes = slice(g * GROUP_ROWS, (g + 1) * GROUP_ROWS)
            got = yr[g * PER_GROUP:(g + 1) * PER_GROUP, :, c].reshape(GROUP_ROWS, 512)
            total = acc[:, c] + dot(mix_hi[:, lanes], got) + dot(mix_lo[:, lanes], got)
            if g < GROUPS - 1:
                acc[:, c] = total
            else:
                out_ref[0, :, c] = total.astype(jnp.bfloat16)

    for t, (src, dst) in enumerate(heads):
        wait_for(dst.at[pl.ds(0, ROWS * (N_SP - 1))], head_send.at[t])
    for i in range(2):
        wait_for(proj_a.at[three, half_rows], proj_send.at[i])
        wait_for(proj_a.at[three, half_rows], relay_send.at[i])
        wait_for(o_buf.at[three], o_send.at[i])
        wait_for(part_a.at[:, three], r_send.at[i])
    wait_for(xs.at[:, fifteen], d_send)
    wait_for(ys.at[fifteen], y_send)


def body(
    queries, keys, values, proj_weight, residual, norm_gain, route, route_weight,
    w_gate, w_up, w_down,
):
    bf16, f32 = jnp.bfloat16, jnp.float32
    vmem = pltpu.VMEM
    dma = pltpu.SemaphoreType.DMA
    anywhere = pl.BlockSpec(memory_space=pl.ANY)
    inside = pl.BlockSpec(memory_space=pltpu.VMEM)
    scratch = [
        vmem((LENGTH, HEAD), bf16), vmem((LENGTH, HEAD), bf16), vmem((LENGTH, HEAD), bf16),
        vmem((LENGTH, LENGTH), bf16), vmem((2 * TILE, HEAD), f32),
        vmem((2, 2 * TILE, TILE), bf16), vmem((2, 2 * TILE, TILE), f32), vmem((TILE, TILE + HEAD), bf16),
        vmem((SIDE, SIDE, ROWS, HEAD), bf16),
        vmem((SIDE, ROWS, 512), bf16), vmem((SIDE, ROWS, 512), bf16),
        vmem((SIDE, ROWS, HALF), bf16), vmem((SIDE, ROWS, HALF), bf16),
        vmem((2, SIDE, ROWS, CHUNK), bf16), vmem((2, SIDE, ROWS, CHUNK), bf16),
        vmem((2, SIDE, ROWS, CHUNK), bf16), vmem((2, SIDE, ROWS, CHUNK), bf16),
        vmem((ROWS, WIDTH), bf16), vmem((ROWS, WIDTH), f32),
        vmem((N_SP * CAP, ROWS), bf16), vmem((ROWS, N_SP * CAP), bf16), vmem((ROWS, N_SP * CAP), bf16),
        vmem((CHUNKS, N_SP, CAP, CHUNK), bf16), vmem((CHUNKS, N_SP, CAP, CHUNK), bf16),
        vmem((N_SP, CAP, WIDTH), bf16), vmem((N_SP, CAP, WIDTH), bf16),
        vmem((N_SP * CAP, CHUNK), bf16), vmem((N_SP * CAP, HEAD), f32),
        vmem((N_SP * CAP, FFE), f32), vmem((N_SP * CAP, FFE), f32),
        vmem((GROUP_ROWS, FFE), bf16),
        vmem((WIDTH, FFE), bf16), vmem((WIDTH, FFE), bf16), vmem((FFE, WIDTH), bf16),
        dma((6,)), dma((3,)), dma((3,)), dma((2,)), dma((2,)), dma((2,)), dma((2,)),
        dma((2,)), dma((SIDE,)), dma, dma((2,)), dma((2,)), dma((2,)),
        dma, dma((CHUNKS - 1 + GROUPS,)), dma, dma((GROUPS,)),
    ]
    return pl.pallas_call(
        body_kernel,
        out_shape=jax.ShapeDtypeStruct((1, ROWS, WIDTH), bf16),
        in_specs=[anywhere] * 5 + [inside] * 3 + [anywhere] * 3,
        out_specs=inside,
        scratch_shapes=scratch,
        compiler_params=pltpu.CompilerParams(
            collective_id=0, has_side_effects=True, vmem_limit_bytes=56 * 1024 * 1024
        ),
        name="layer",
    )(
        queries, keys, values, proj_weight, residual, norm_gain.reshape(1, WIDTH),
        jnp.swapaxes(route, 1, 2), jnp.swapaxes(route_weight, 1, 2), w_gate, w_up, w_down,
    )


def solution(mesh):
    return jax.shard_map(
        body,
        mesh=mesh,
        in_specs=(
            P("dp", "sp", None),
            P("dp", "sp", None),
            P("dp", "sp", None),
            P("sp", None),
            P("dp", "sp", None),
            P(),
            P("dp", "sp", None),
            P("dp", "sp", None),
            P("sp", None, None),
            P("sp", None, None),
            P("sp", None, None),
        ),
        out_specs=P("dp", "sp", None),
        check_vma=False,
    )
```

```python
import functools
import math

import jax
import jax.numpy as jnp
from jax import lax
from jax.experimental import pallas as pl
from jax.experimental.pallas import tpu as pltpu
from jax.sharding import PartitionSpec as P

MESH = pl.DeviceIdType.MESH
EPS = 1e-06
SIDE = 4
N_SP = 16
ROWS = 128
HEAD = 128
LENGTH = 2048
WIDTH = 2048
FFE = 1024
COLS_Z = 1024
COLS_Y = WIDTH - COLS_Z
PIECES = (("y", COLS_Z, 512), ("z", 0, 512), ("y", COLS_Z + 512, 512), ("z", 512, 512))
EARLY = 2
CAP = 32
TILE = 256
LOG2E = 1.0 / math.log(2.0)

SHIFTS = (
    (1, 2), (3, 2), (2, 1), (2, 3),
    (2, 2), (2, 0), (0, 2), (0, 0),
    (1, 1), (3, 3), (1, 3), (3, 1),
    (1, 0), (3, 0), (0, 1), (0, 3),
)
OWN = SHIFTS.index((0, 0))
GROUPS = 4
PER_GROUP = 4
GROUP_ROWS = PER_GROUP * CAP


def dot(a, b):
    return jnp.dot(a, b, preferred_element_type=jnp.float32)


def body_kernel(
    q_hbm, k_hbm, v_hbm, proj_hbm, res_hbm, gain_ref, route_ref, rw_ref,
    wg_hbm, wu_hbm, wd_hbm,
    out_ref,
    qh, kh, vh, w_att, carry, softer, power, tri, o_buf, oa, ob, proj_a, proj_b,
    part0, part1, part2, part3, sum0, sum1, sum2, sum3, res, acc, pick, mix_hi, mix_lo,
    xs0, xs1, xs2, xs3, xr0, xr1, xr2, xr3, ys, yr, scaled, squares, gate_acc, up_acc, hid, wg, wu, wd,
    local_sem, head_send, head_recv, proj_send, proj_recv, relay_send, relay_recv,
    o_send, oa_recv, ob_recv, r_send, r_recv, d_send, d_recv, group_recv, y_send, y_recv,
):
    parts, sums = (part0, part1, part2, part3), (sum0, sum1, sum2, sum3)
    xs, xr = (xs0, xs1, xs2, xs3), (xr0, xr1, xr2, xr3)
    me = lax.axis_index("sp")
    dp = lax.axis_index("dp")
    z = me // SIDE
    y = me % SIDE
    core = dp % 2
    partner = dp + 1 - 2 * core

    def at(a, b):
        return ((z + a) % SIDE) * SIDE + (y + b) % SIDE

    others = [s for s in SHIFTS if s != (0, 0)]
    line = (2, 1, 3)

    barrier = pltpu.get_barrier_semaphore()
    for a, b in others:
        pl.semaphore_signal(barrier, inc=1, device_id={"sp": at(a, b)}, device_id_type=MESH)
    pl.semaphore_signal(barrier, inc=1, device_id={"dp": partner}, device_id_type=MESH)

    def local(src, dst, sem):
        copy = pltpu.make_async_copy(src, dst, sem)
        copy.start()
        return copy

    def remote(src, dst, send, recv, peer, axis="sp"):
        pltpu.make_async_remote_copy(
            src_ref=src, dst_ref=dst, send_sem=send, recv_sem=recv,
            device_id={axis: peer}, device_id_type=MESH,
        ).start()

    def wait_for(ref, sem):
        pltpu.make_async_copy(ref, ref, sem).wait()

    my_rows = pl.ds(pl.multiple_of(me * ROWS, ROWS), ROWS)
    core_rows = pl.ds(pl.multiple_of(core * (ROWS // 2), ROWS // 2), ROWS // 2)

    def cols(peer):
        return pl.ds(pl.multiple_of(peer * HEAD, HEAD), HEAD)

    heads = ((k_hbm, kh), (q_hbm, qh), (v_hbm, vh))
    for t, (src, dst) in enumerate(heads):
        local(src.at[0, :, cols(me)], dst.at[my_rows], head_recv.at[t])
    loads = [
        local(proj_hbm.at[:, pl.ds(0, COLS_Z)], proj_a.at[y], local_sem.at[4]),
        local(proj_hbm.at[:, pl.ds(COLS_Z, COLS_Y)], proj_b.at[z], local_sem.at[5]),
    ]

    pl.semaphore_wait(barrier, N_SP)

    def send_heads(t, a, b):
        src, dst = heads[t]
        peer = at(a, b)
        remote(src.at[0, :, cols(peer)], dst.at[my_rows], head_send.at[t], head_recv.at[t], peer)

    for t in range(3):
        for a, b in others:
            send_heads(t, a, b)
    for s in line:
        remote(proj_hbm.at[core_rows, pl.ds(0, COLS_Z)], proj_a.at[y, core_rows],
               proj_send.at[0], proj_recv.at[0], at(0, s))
    for s in line:
        remote(proj_hbm.at[core_rows, pl.ds(COLS_Z, COLS_Y)], proj_b.at[z, core_rows],
               proj_send.at[1], proj_recv.at[1], at(s, 0))
    loads += [
        local(res_hbm.at[0], res, local_sem.at[0]),
        local(wg_hbm.at[0], wg, local_sem.at[1]),
        local(wu_hbm.at[0], wu, local_sem.at[2]),
        local(wd_hbm.at[0], wd, local_sem.at[3]),
    ]

    j = lax.broadcasted_iota(jnp.int32, (TILE, TILE + HEAD), 0)
    s = lax.broadcasted_iota(jnp.int32, (TILE, TILE + HEAD), 1)
    tri[...] = jnp.where((j > s) | (s >= TILE), 1.0, 0.0).astype(jnp.bfloat16)

    @pl.loop(0, LENGTH // 64)
    def _(i):
        w_att[pl.ds(pl.multiple_of(i * 64, 64), 64), :] = jnp.zeros((64, LENGTH), jnp.bfloat16)

    slots = N_SP * CAP
    lane = lax.broadcasted_iota(jnp.int32, (ROWS, slots), 1)
    place = lane // CAP
    expert = jnp.zeros((ROWS, slots), jnp.int32)
    for i, (a, b) in enumerate(SHIFTS):
        expert = jnp.where(place == i, at(a, b), expert)
    zeros = jnp.zeros((6, ROWS), jnp.float32)
    route = jnp.concatenate([route_ref[0].astype(jnp.float32), zeros], axis=0).T
    share = jnp.concatenate([rw_ref[0], zeros], axis=0).T
    expert = expert.astype(jnp.float32)
    first = route[:, 0:1] == expert
    second = route[:, 1:2] == expert
    named = jnp.where(first | second, 1.0, 0.0)
    r0 = lax.broadcasted_iota(jnp.int32, (ROWS, ROWS), 0)
    r1 = lax.broadcasted_iota(jnp.int32, (ROWS, ROWS), 1)
    before = jnp.where(r1 < r0, 1.0, 0.0).astype(jnp.bfloat16)
    slot = dot(before, named.astype(jnp.bfloat16))
    held = jnp.where(slot == (lane - place * CAP).astype(jnp.float32), named, 0.0)
    pick[...] = held.T.astype(jnp.bfloat16)
    mix = held * jnp.where(first, share[:, 0:1], share[:, 1:2])
    high = mix.astype(jnp.bfloat16)
    mix_hi[...] = high
    mix_lo[...] = (mix - high.astype(jnp.float32)).astype(jnp.bfloat16)

    wait_for(kh, head_recv.at[0])
    wait_for(qh, head_recv.at[1])
    scale = HEAD ** (-0.5)

    causal = lax.broadcasted_iota(jnp.int32, (TILE, TILE), 1) < lax.broadcasted_iota(
        jnp.int32, (TILE, TILE), 0
    )

    def soften(base, lines, k0, which, diagonal):
        rows = slice(*lines)
        u = lax.dot_general(
            qh[pl.ds(pl.multiple_of(base + lines[0], TILE), lines[1] - lines[0]), :],
            kh[pl.ds(k0, TILE), :], (((1,), (1,)), ((), ())),
            preferred_element_type=jnp.float32,
        ) * scale
        low = jnp.log(1.0 + jnp.exp2(jnp.abs(u) * -LOG2E))
        soft = jnp.maximum(u, 0.0) + low
        if diagonal:
            soft = jnp.where(causal, soft, 0.0)
        softer[which, rows, :] = soft.astype(jnp.bfloat16)
        power[which, rows, :] = jnp.minimum(u, 0.0) - low

    def weigh(base, lines, k0, which, diagonal, fresh):
        rows = slice(*lines)
        sums = dot(softer[which, rows, :], tri[...])
        less = sums[:, :TILE]
        total = sums[:, TILE:]
        if not fresh:
            later = carry[rows, :]
            less = less + jnp.concatenate([later, later], axis=1)
            total = total + later
        weight = jnp.exp2((power[which, rows, :] - less) * LOG2E)
        if diagonal:
            weight = jnp.where(causal, weight, 0.0)
        place = pl.ds(pl.multiple_of(base + lines[0], TILE), lines[1] - lines[0])
        w_att[place, pl.ds(k0, TILE)] = weight.astype(jnp.bfloat16)
        carry[rows, :] = total

    upper, lower, both = (0, TILE), (TILE, 2 * TILE), (0, 2 * TILE)

    def quarter_weights(quarter):
        base = pl.multiple_of(quarter * 512, 512)
        second = pl.multiple_of(base + TILE, TILE)
        soften(base, lower, second, 1, True)
        soften(base, upper, base, 0, True)
        soften(base, lower, base, 0, False)
        weigh(base, lower, second, 1, True, True)
        weigh(base, upper, base, 0, True, True)
        weigh(base, lower, base, 0, False, False)

        @pl.loop(0, quarter)
        def _(i):
            for which in range(2):
                k0 = pl.multiple_of((2 * quarter - 2 * i - 1 - which) * TILE, TILE)
                soften(base, both, k0, which, False)
                weigh(base, both, k0, which, False, False)

    def quarter_values(i):
        quarter = (z + 1 + i) % SIDE
        rows = pl.ds(pl.multiple_of(quarter * 512, 512), 512)
        o_buf[quarter] = dot(w_att[rows, :], vh[...]).astype(jnp.bfloat16).reshape(SIDE, ROWS, HEAD)
        if i < SIDE - 1:
            remote(o_buf.at[quarter], ob.at[:, :, cols(z)], o_send.at[1], ob_recv, quarter * SIDE + y)
        else:
            ob[:, :, cols(z)] = o_buf[z]
        for s in line:
            peer_y = (y + s) % SIDE
            remote(o_buf.at[quarter, peer_y], oa.at[quarter, :, cols(y)], o_send.at[0],
                   oa_recv.at[quarter], z * SIDE + peer_y)
        oa[quarter, :, cols(y)] = o_buf[quarter, y]

    three = pl.ds(0, SIDE - 1)
    half_rows = pl.ds(0, ROWS // 2)

    def relay():
        for index, (weight, mine) in enumerate(((proj_a, y), (proj_b, z))):
            wait_for(weight.at[three, half_rows], proj_recv.at[index])
            for s in line:
                piece = weight.at[(mine + s) % SIDE, core_rows]
                remote(piece, piece, relay_send.at[index], relay_recv.at[index], partner, "dp")

    def project_z(i):
        quarter = (z + 1 + i) % SIDE
        wait_for(oa.at[0, :, pl.ds(0, 3 * HEAD)], oa_recv.at[quarter])
        left = oa[quarter]
        for k, (axis, start, width) in enumerate(PIECES):
            if axis == "y":
                continue
            for n in range(width // TILE):
                right = proj_a[:, :, start + n * TILE:start + (n + 1) * TILE].reshape(512, TILE)
                parts[k][quarter, :, n * TILE:(n + 1) * TILE] = dot(left, right).astype(jnp.bfloat16)
            if i < SIDE - 1:
                remote(parts[k].at[quarter], sums[k].at[z], r_send.at[k], r_recv.at[k], quarter * SIDE + y)
            else:
                sums[k][z] = parts[k][z]

    def project_y(k):
        start, width = PIECES[k][1] - COLS_Z, PIECES[k][2]
        for n in range(width // TILE):
            right = proj_b[:, :, start + n * TILE:start + (n + 1) * TILE].reshape(512, TILE)
            block = dot(ob[...].reshape(512, 512), right).astype(jnp.bfloat16)
            parts[k][:, :, n * TILE:(n + 1) * TILE] = block.reshape(SIDE, ROWS, TILE)
        for s in line:
            peer_y = (y + s) % SIDE
            remote(parts[k].at[peer_y], sums[k].at[y], r_send.at[k], r_recv.at[k], z * SIDE + peer_y)
        sums[k][y] = parts[k][y]

    quarter_weights((z + 1) % SIDE)
    quarter_weights((z + 2) % SIDE)
    wait_for(vh, head_recv.at[2])
    quarter_values(0)
    quarter_values(1)
    quarter_weights((z + 3) % SIDE)
    quarter_values(2)
    relay()
    quarter_weights(z)
    quarter_values(3)
    loads[0].wait()
    loads[1].wait()
    wait_for(proj_b.at[three, half_rows], relay_recv.at[1])
    wait_for(ob.at[:, :, pl.ds(0, 3 * HEAD)], ob_recv)
    project_y(0)
    wait_for(proj_a.at[three, half_rows], relay_recv.at[0])
    project_z(0)
    project_y(2)
    project_z(1)
    project_z(2)
    project_z(3)

    last = len(PIECES) - 1

    def dispatch(k, g, sem):
        for i in range(g * PER_GROUP, (g + 1) * PER_GROUP):
            if i != OWN:
                remote(xs[k].at[i], xr[k].at[i], d_send.at[k], sem, at(*SHIFTS[i]))

    loads[2].wait()
    for k, (axis, start, width) in enumerate(PIECES):
        wait_for(sums[k].at[three], r_recv.at[k])
        for n in range(width // TILE):
            c = slice(n * TILE, (n + 1) * TILE)
            place = slice(start + n * TILE, start + (n + 1) * TILE)
            total = res[:, place].astype(jnp.float32)
            for i in range(SIDE):
                total = total + sums[k][i, :, c].astype(jnp.float32)
            stream = total.astype(jnp.bfloat16)
            acc[:, place] = stream.astype(jnp.float32)
            rows = dot(pick[...], stream).astype(jnp.bfloat16)
            xs[k][:, :, c] = rows.reshape(N_SP, CAP, TILE)
        if k < EARLY:
            for g in range(GROUPS):
                dispatch(k, g, d_recv.at[k])
        xr[k][OWN] = xs[k][OWN]
        if k == EARLY:
            dispatch(k, 0, group_recv.at[k - EARLY, 0])
    for g in range(GROUPS):
        for k in range(EARLY, last + 1):
            if g > 0 or k > EARLY:
                dispatch(k, g, group_recv.at[k - EARLY, g])

    for load in loads[3:]:
        load.wait()
    fifteen = pl.ds(0, N_SP - 1)
    for k, (axis, start, width) in enumerate(PIECES[:EARLY]):
        wait_for(xr[k].at[fifteen], d_recv.at[k])

        @pl.loop(0, GROUPS)
        def _(g):
            rows = xr[k][pl.ds(g * PER_GROUP, PER_GROUP)].astype(jnp.float32).reshape(GROUP_ROWS, width)
            r = pl.ds(pl.multiple_of(g * GROUP_ROWS, GROUP_ROWS), GROUP_ROWS)
            scaled[r, :width] = (rows * gain_ref[:, start:start + width]).astype(jnp.bfloat16)
            square = jnp.sum(rows * rows, axis=-1, keepdims=True)
            square = jnp.broadcast_to(square, (GROUP_ROWS, HEAD))
            squares[r, :] = square if k == 0 else squares[r, :] + square

        @pl.loop(0, FFE // (2 * TILE))
        def _(n):
            for weight, total in ((wg, gate_acc), (wu, up_acc)):
                for half in range(2):
                    c = pl.ds(pl.multiple_of(n * (2 * TILE) + half * TILE, TILE), TILE)
                    new = dot(scaled[:, :width], weight[start:start + width, c])
                    total[:, c] = new if k == 0 else total[:, c] + new

    def remote_count(g):
        return PER_GROUP - (1 if OWN // PER_GROUP == g else 0)

    for g in range(GROUPS):
        mine = slice(g * PER_GROUP, (g + 1) * PER_GROUP)
        lines = slice(g * GROUP_ROWS, (g + 1) * GROUP_ROWS)
        square = squares[lines, 0:1]
        late = []
        for k in range(EARLY, last + 1):
            axis, start, width = PIECES[k]
            wait_for(xr[k].at[pl.ds(g * PER_GROUP, remote_count(g))], group_recv.at[k - EARLY, g])
            rows = xr[k][mine].astype(jnp.float32).reshape(GROUP_ROWS, width)
            square = square + jnp.sum(rows * rows, axis=-1, keepdims=True)
            at_col = (k - EARLY) * 512
            scaled[lines, at_col:at_col + width] = (rows * gain_ref[:, start:start + width]).astype(jnp.bfloat16)
            late.append((at_col, start, width))
        factor = lax.rsqrt(square * (1.0 / WIDTH) + EPS)
        norm = jnp.broadcast_to(factor, (GROUP_ROWS, TILE))
        for n in range(FFE // TILE):
            c = slice(n * TILE, (n + 1) * TILE)
            gate, upper = gate_acc[lines, c], up_acc[lines, c]
            for at_col, start, width in late:
                x = scaled[lines, at_col:at_col + width]
                gate = gate + dot(x, wg[start:start + width, c])
                upper = upper + dot(x, wu[start:start + width, c])
            gate, upper = gate * norm, upper * norm
            hid[:, c] = (gate / (1.0 + jnp.exp(-gate)) * upper).astype(jnp.bfloat16)

        for n in range(WIDTH // TILE):
            c = slice(n * TILE, (n + 1) * TILE)
            result = dot(hid[...], wd[:, c]).astype(jnp.bfloat16)
            ys[mine, :, c] = result.reshape(PER_GROUP, CAP, TILE)

        for i in range(g * PER_GROUP, (g + 1) * PER_GROUP):
            if i == OWN:
                yr[i] = ys[i]
            else:
                a, b = SHIFTS[i]
                remote(ys.at[i], yr.at[i], y_send, y_recv.at[g], at(-a, -b))

    for g in range(GROUPS):
        wait_for(yr.at[pl.ds(g * PER_GROUP, remote_count(g))], y_recv.at[g])

        for n in range(WIDTH // 512):
            c = slice(n * 512, (n + 1) * 512)
            lanes = slice(g * GROUP_ROWS, (g + 1) * GROUP_ROWS)
            got = yr[g * PER_GROUP:(g + 1) * PER_GROUP, :, c].reshape(GROUP_ROWS, 512)
            total = acc[:, c] + dot(mix_hi[:, lanes], got) + dot(mix_lo[:, lanes], got)
            if g < GROUPS - 1:
                acc[:, c] = total
            else:
                out_ref[0, :, c] = total.astype(jnp.bfloat16)

    for t, (src, dst) in enumerate(heads):
        wait_for(dst.at[pl.ds(0, ROWS * (N_SP - 1))], head_send.at[t])
    for i in range(2):
        weight = (proj_a, proj_b)[i]
        wait_for(weight.at[three, half_rows], proj_send.at[i])
        wait_for(weight.at[three, half_rows], relay_send.at[i])
        wait_for(o_buf.at[three], o_send.at[i])
    for k in range(len(PIECES)):
        wait_for(parts[k].at[three], r_send.at[k])
        wait_for(xs[k].at[fifteen], d_send.at[k])
    wait_for(ys.at[fifteen], y_send)


def body(
    queries, keys, values, proj_weight, residual, norm_gain, route, route_weight,
    w_gate, w_up, w_down,
):
    bf16, f32 = jnp.bfloat16, jnp.float32
    vmem = pltpu.VMEM
    dma = pltpu.SemaphoreType.DMA
    anywhere = pl.BlockSpec(memory_space=pl.ANY)
    inside = pl.BlockSpec(memory_space=pltpu.VMEM)
    scratch = [
        vmem((LENGTH, HEAD), bf16), vmem((LENGTH, HEAD), bf16), vmem((LENGTH, HEAD), bf16),
        vmem((LENGTH, LENGTH), bf16), vmem((2 * TILE, HEAD), f32),
        vmem((2, 2 * TILE, TILE), bf16), vmem((2, 2 * TILE, TILE), f32), vmem((TILE, TILE + HEAD), bf16),
        vmem((SIDE, SIDE, ROWS, HEAD), bf16),
        vmem((SIDE, ROWS, 512), bf16), vmem((SIDE, ROWS, 512), bf16),
        vmem((SIDE, ROWS, COLS_Z), bf16), vmem((SIDE, ROWS, COLS_Y), bf16),
    ]
    scratch += [vmem((SIDE, ROWS, width), bf16) for axis, start, width in PIECES] * 2
    scratch += [
        vmem((ROWS, WIDTH), bf16), vmem((ROWS, WIDTH), f32),
        vmem((N_SP * CAP, ROWS), bf16), vmem((ROWS, N_SP * CAP), bf16), vmem((ROWS, N_SP * CAP), bf16),
    ]
    scratch += [vmem((N_SP, CAP, width), bf16) for axis, start, width in PIECES] * 2
    scratch += [
        vmem((N_SP, CAP, WIDTH), bf16), vmem((N_SP, CAP, WIDTH), bf16),
        vmem((N_SP * CAP, 1024), bf16), vmem((N_SP * CAP, HEAD), f32),
        vmem((N_SP * CAP, FFE), f32), vmem((N_SP * CAP, FFE), f32),
        vmem((GROUP_ROWS, FFE), bf16),
        vmem((WIDTH, FFE), bf16), vmem((WIDTH, FFE), bf16), vmem((FFE, WIDTH), bf16),
        dma((6,)), dma((3,)), dma((3,)), dma((2,)), dma((2,)), dma((2,)), dma((2,)),
        dma((2,)), dma((SIDE,)), dma, dma((4,)), dma((4,)),
        dma((4,)), dma((EARLY,)), dma((2, GROUPS)), dma, dma((GROUPS,)),
    ]
    return pl.pallas_call(
        body_kernel,
        out_shape=pltpu.VMEM((1, ROWS, WIDTH), bf16),
        in_specs=[anywhere] * 5 + [inside] * 3 + [anywhere] * 3,
        out_specs=inside,
        scratch_shapes=scratch,
        compiler_params=pltpu.CompilerParams(
            collective_id=0, has_side_effects=True, vmem_limit_bytes=56 * 1024 * 1024
        ),
        name="layer",
    )(
        queries, keys, values, proj_weight, residual, norm_gain.reshape(1, WIDTH),
        jnp.swapaxes(route, 1, 2), jnp.swapaxes(route_weight, 1, 2), w_gate, w_up, w_down,
    )


def solution(mesh):
    return jax.shard_map(
        body,
        mesh=mesh,
        in_specs=(
            P("dp", "sp", None),
            P("dp", "sp", None),
            P("dp", "sp", None),
            P("sp", None),
            P("dp", "sp", None),
            P(),
            P("dp", "sp", None),
            P("dp", "sp", None),
            P("sp", None, None),
            P("sp", None, None),
            P("sp", None, None),
        ),
        out_specs=P("dp", "sp", None),
        check_vma=False,
    )
```

```python
import functools
import math

import jax
import jax.numpy as jnp
from jax import lax
from jax.experimental import pallas as pl
from jax.experimental.pallas import tpu as pltpu
from jax.sharding import PartitionSpec as P

MESH = pl.DeviceIdType.MESH
EPS = 1e-06
SIDE = 4
N_SP = 16
ROWS = 128
HEAD = 128
LENGTH = 2048
WIDTH = 2048
FFE = 1024
COLS_Z = 1024
COLS_Y = WIDTH - COLS_Z
PIECES = (("y", COLS_Z, 512), ("z", 0, 512), ("y", COLS_Z + 512, 512), ("z", 512, 512))
EARLY = 2
CAP = 32
TILE = 256
LOG2E = 1.0 / math.log(2.0)

SHIFTS = (
    (1, 2), (3, 2), (2, 1), (2, 3),
    (2, 2), (2, 0), (0, 2), (0, 0),
    (1, 1), (3, 3), (1, 3), (3, 1),
    (1, 0), (3, 0), (0, 1), (0, 3),
)
OWN = SHIFTS.index((0, 0))
GROUPS = 4
PER_GROUP = 4
GROUP_ROWS = PER_GROUP * CAP


def dot(a, b):
    return jnp.dot(a, b, preferred_element_type=jnp.float32)


def body_kernel(
    q_hbm, k_hbm, v_hbm, proj_hbm, res_hbm, gain_ref, route_ref, rw_ref,
    wg_hbm, wu_hbm, wd_hbm,
    out_ref,
    qh, kh, vh, w_att, carry, softer, power, tri, o_buf, oa, ob, proj_a, proj_b,
    part0, part1, part2, part3, sum0, sum1, sum2, sum3, res, acc, pick, mix_hi, mix_lo,
    xs0, xs1, xs2, xs3, xr0, xr1, xr2, xr3, ys, yr, scaled, squares, gate_acc, up_acc, hid, wg, wu, wd,
    local_sem, head_send, head_recv, proj_send, proj_recv, relay_send, relay_recv,
    o_send, oa_recv, ob_recv, r_send, r_recv, d_send, d_recv, group_recv, y_send, y_recv,
):
    parts, sums = (part0, part1, part2, part3), (sum0, sum1, sum2, sum3)
    xs, xr = (xs0, xs1, xs2, xs3), (xr0, xr1, xr2, xr3)
    me = lax.axis_index("sp")
    dp = lax.axis_index("dp")
    z = me // SIDE
    y = me % SIDE
    core = dp % 2
    partner = dp + 1 - 2 * core

    def at(a, b):
        return ((z + a) % SIDE) * SIDE + (y + b) % SIDE

    others = [s for s in SHIFTS if s != (0, 0)]
    line = (2, 1, 3)

    barrier = pltpu.get_barrier_semaphore()
    for a, b in others:
        pl.semaphore_signal(barrier, inc=1, device_id={"sp": at(a, b)}, device_id_type=MESH)
    pl.semaphore_signal(barrier, inc=1, device_id={"dp": partner}, device_id_type=MESH)

    def local(src, dst, sem):
        copy = pltpu.make_async_copy(src, dst, sem)
        copy.start()
        return copy

    def remote(src, dst, send, recv, peer, axis="sp"):
        pltpu.make_async_remote_copy(
            src_ref=src, dst_ref=dst, send_sem=send, recv_sem=recv,
            device_id={axis: peer}, device_id_type=MESH,
        ).start()

    def wait_for(ref, sem):
        pltpu.make_async_copy(ref, ref, sem).wait()

    my_rows = pl.ds(pl.multiple_of(me * ROWS, ROWS), ROWS)
    core_rows = pl.ds(pl.multiple_of(core * (ROWS // 2), ROWS // 2), ROWS // 2)

    def cols(peer):
        return pl.ds(pl.multiple_of(peer * HEAD, HEAD), HEAD)

    heads = ((k_hbm, kh), (q_hbm, qh), (v_hbm, vh))
    for t, (src, dst) in enumerate(heads):
        local(src.at[0, :, cols(me)], dst.at[my_rows], head_recv.at[t])
    loads = [
        local(proj_hbm.at[:, pl.ds(0, COLS_Z)], proj_a.at[y], local_sem.at[4]),
        local(proj_hbm.at[:, pl.ds(COLS_Z, COLS_Y)], proj_b.at[z], local_sem.at[5]),
    ]

    pl.semaphore_wait(barrier, N_SP)

    def send_heads(t, a, b):
        src, dst = heads[t]
        peer = at(a, b)
        remote(src.at[0, :, cols(peer)], dst.at[my_rows], head_send.at[t], head_recv.at[t], peer)

    for t in range(3):
        for a, b in others:
            send_heads(t, a, b)
    loads += [
        local(res_hbm.at[0], res, local_sem.at[0]),
        local(wg_hbm.at[0], wg, local_sem.at[1]),
        local(wu_hbm.at[0], wu, local_sem.at[2]),
        local(wd_hbm.at[0], wd, local_sem.at[3]),
    ]

    j = lax.broadcasted_iota(jnp.int32, (TILE, TILE + HEAD), 0)
    s = lax.broadcasted_iota(jnp.int32, (TILE, TILE + HEAD), 1)
    tri[...] = jnp.where((j > s) | (s >= TILE), 1.0, 0.0).astype(jnp.bfloat16)

    @pl.loop(0, LENGTH // 64)
    def _(i):
        w_att[pl.ds(pl.multiple_of(i * 64, 64), 64), :] = jnp.zeros((64, LENGTH), jnp.bfloat16)

    slots = N_SP * CAP
    lane = lax.broadcasted_iota(jnp.int32, (ROWS, slots), 1)
    place = lane // CAP
    expert = jnp.zeros((ROWS, slots), jnp.int32)
    for i, (a, b) in enumerate(SHIFTS):
        expert = jnp.where(place == i, at(a, b), expert)
    zeros = jnp.zeros((6, ROWS), jnp.float32)
    route = jnp.concatenate([route_ref[0].astype(jnp.float32), zeros], axis=0).T
    share = jnp.concatenate([rw_ref[0], zeros], axis=0).T
    expert = expert.astype(jnp.float32)
    first = route[:, 0:1] == expert
    second = route[:, 1:2] == expert
    named = jnp.where(first | second, 1.0, 0.0)
    r0 = lax.broadcasted_iota(jnp.int32, (ROWS, ROWS), 0)
    r1 = lax.broadcasted_iota(jnp.int32, (ROWS, ROWS), 1)
    before = jnp.where(r1 < r0, 1.0, 0.0).astype(jnp.bfloat16)
    slot = dot(before, named.astype(jnp.bfloat16))
    held = jnp.where(slot == (lane - place * CAP).astype(jnp.float32), named, 0.0)
    pick[...] = held.T.astype(jnp.bfloat16)
    mix = held * jnp.where(first, share[:, 0:1], share[:, 1:2])
    high = mix.astype(jnp.bfloat16)
    mix_hi[...] = high
    mix_lo[...] = (mix - high.astype(jnp.float32)).astype(jnp.bfloat16)

    wait_for(kh, head_recv.at[0])
    for s in line:
        remote(proj_hbm.at[core_rows, pl.ds(0, COLS_Z)], proj_a.at[y, core_rows],
               proj_send.at[0], proj_recv.at[0], at(0, s))
    for s in line:
        remote(proj_hbm.at[core_rows, pl.ds(COLS_Z, COLS_Y)], proj_b.at[z, core_rows],
               proj_send.at[1], proj_recv.at[1], at(s, 0))
    wait_for(qh, head_recv.at[1])
    scale = HEAD ** (-0.5)

    causal = lax.broadcasted_iota(jnp.int32, (TILE, TILE), 1) < lax.broadcasted_iota(
        jnp.int32, (TILE, TILE), 0
    )

    def soften(base, lines, k0, which, diagonal):
        rows = slice(*lines)
        u = lax.dot_general(
            qh[pl.ds(pl.multiple_of(base + lines[0], TILE), lines[1] - lines[0]), :],
            kh[pl.ds(k0, TILE), :], (((1,), (1,)), ((), ())),
            preferred_element_type=jnp.float32,
        ) * scale
        low = jnp.log(1.0 + jnp.exp2(jnp.abs(u) * -LOG2E))
        soft = jnp.maximum(u, 0.0) + low
        if diagonal:
            soft = jnp.where(causal, soft, 0.0)
        softer[which, rows, :] = soft.astype(jnp.bfloat16)
        power[which, rows, :] = jnp.minimum(u, 0.0) - low

    def weigh(base, lines, k0, which, diagonal, fresh):
        rows = slice(*lines)
        sums = dot(softer[which, rows, :], tri[...])
        less = sums[:, :TILE]
        total = sums[:, TILE:]
        if not fresh:
            later = carry[rows, :]
            less = less + jnp.concatenate([later, later], axis=1)
            total = total + later
        weight = jnp.exp2((power[which, rows, :] - less) * LOG2E)
        if diagonal:
            weight = jnp.where(causal, weight, 0.0)
        place = pl.ds(pl.multiple_of(base + lines[0], TILE), lines[1] - lines[0])
        w_att[place, pl.ds(k0, TILE)] = weight.astype(jnp.bfloat16)
        carry[rows, :] = total

    upper, lower, both = (0, TILE), (TILE, 2 * TILE), (0, 2 * TILE)

    def quarter_weights(quarter):
        base = pl.multiple_of(quarter * 512, 512)
        second = pl.multiple_of(base + TILE, TILE)
        soften(base, lower, second, 1, True)
        soften(base, upper, base, 0, True)
        soften(base, lower, base, 0, False)
        weigh(base, lower, second, 1, True, True)
        weigh(base, upper, base, 0, True, True)
        weigh(base, lower, base, 0, False, False)

        @pl.loop(0, quarter)
        def _(i):
            for which in range(2):
                k0 = pl.multiple_of((2 * quarter - 2 * i - 1 - which) * TILE, TILE)
                soften(base, both, k0, which, False)
                weigh(base, both, k0, which, False, False)

    def quarter_values(i):
        quarter = (z + 1 + i) % SIDE
        rows = pl.ds(pl.multiple_of(quarter * 512, 512), 512)
        o_buf[quarter] = dot(w_att[rows, :], vh[...]).astype(jnp.bfloat16).reshape(SIDE, ROWS, HEAD)
        if i < SIDE - 1:
            remote(o_buf.at[quarter], ob.at[:, :, cols(z)], o_send.at[1], ob_recv, quarter * SIDE + y)
        else:
            ob[:, :, cols(z)] = o_buf[z]
        for s in line:
            peer_y = (y + s) % SIDE
            remote(o_buf.at[quarter, peer_y], oa.at[quarter, :, cols(y)], o_send.at[0],
                   oa_recv.at[quarter], z * SIDE + peer_y)
        oa[quarter, :, cols(y)] = o_buf[quarter, y]

    three = pl.ds(0, SIDE - 1)
    half_rows = pl.ds(0, ROWS // 2)

    def relay():
        for index, (weight, mine) in enumerate(((proj_a, y), (proj_b, z))):
            wait_for(weight.at[three, half_rows], proj_recv.at[index])
            for s in line:
                piece = weight.at[(mine + s) % SIDE, core_rows]
                remote(piece, piece, relay_send.at[index], relay_recv.at[index], partner, "dp")

    def project_z(i):
        quarter = (z + 1 + i) % SIDE
        wait_for(oa.at[0, :, pl.ds(0, 3 * HEAD)], oa_recv.at[quarter])
        left = oa[quarter]
        for k, (axis, start, width) in enumerate(PIECES):
            if axis == "y":
                continue
            for n in range(width // TILE):
                right = proj_a[:, :, start + n * TILE:start + (n + 1) * TILE].reshape(512, TILE)
                parts[k][quarter, :, n * TILE:(n + 1) * TILE] = dot(left, right).astype(jnp.bfloat16)
            if i < SIDE - 1:
                remote(parts[k].at[quarter], sums[k].at[z], r_send.at[k], r_recv.at[k], quarter * SIDE + y)
            else:
                sums[k][z] = parts[k][z]

    def project_y(k):
        start, width = PIECES[k][1] - COLS_Z, PIECES[k][2]
        for n in range(width // TILE):
            right = proj_b[:, :, start + n * TILE:start + (n + 1) * TILE].reshape(512, TILE)
            block = dot(ob[...].reshape(512, 512), right).astype(jnp.bfloat16)
            parts[k][:, :, n * TILE:(n + 1) * TILE] = block.reshape(SIDE, ROWS, TILE)
        for s in line:
            peer_y = (y + s) % SIDE
            remote(parts[k].at[peer_y], sums[k].at[y], r_send.at[k], r_recv.at[k], z * SIDE + peer_y)
        sums[k][y] = parts[k][y]

    quarter_weights((z + 1) % SIDE)
    quarter_weights((z + 2) % SIDE)
    wait_for(vh, head_recv.at[2])
    quarter_values(0)
    quarter_values(1)
    quarter_weights((z + 3) % SIDE)
    quarter_values(2)
    relay()
    quarter_weights(z)
    quarter_values(3)
    loads[0].wait()
    loads[1].wait()
    wait_for(proj_b.at[three, half_rows], relay_recv.at[1])
    wait_for(ob.at[:, :, pl.ds(0, 3 * HEAD)], ob_recv)
    project_y(0)
    wait_for(proj_a.at[three, half_rows], relay_recv.at[0])
    project_z(0)
    project_y(2)
    project_z(1)
    project_z(2)
    project_z(3)

    last = len(PIECES) - 1

    def dispatch(k, g, sem):
        for i in range(g * PER_GROUP, (g + 1) * PER_GROUP):
            if i != OWN:
                remote(xs[k].at[i], xr[k].at[i], d_send.at[k], sem, at(*SHIFTS[i]))

    loads[2].wait()
    for k, (axis, start, width) in enumerate(PIECES):
        wait_for(sums[k].at[three], r_recv.at[k])
        for n in range(width // TILE):
            c = slice(n * TILE, (n + 1) * TILE)
            place = slice(start + n * TILE, start + (n + 1) * TILE)
            total = res[:, place].astype(jnp.float32)
            for i in range(SIDE):
                total = total + sums[k][i, :, c].astype(jnp.float32)
            stream = total.astype(jnp.bfloat16)
            acc[:, place] = stream.astype(jnp.float32)
            rows = dot(pick[...], stream).astype(jnp.bfloat16)
            xs[k][:, :, c] = rows.reshape(N_SP, CAP, TILE)
        if k < EARLY:
            for g in range(GROUPS):
                dispatch(k, g, d_recv.at[k])
        xr[k][OWN] = xs[k][OWN]
        if k == EARLY:
            dispatch(k, 0, group_recv.at[k - EARLY, 0])
    for g in range(GROUPS):
        for k in range(EARLY, last + 1):
            if g > 0 or k > EARLY:
                dispatch(k, g, group_recv.at[k - EARLY, g])

    for load in loads[3:]:
        load.wait()
    fifteen = pl.ds(0, N_SP - 1)
    for k, (axis, start, width) in enumerate(PIECES[:EARLY]):
        wait_for(xr[k].at[fifteen], d_recv.at[k])

        @pl.loop(0, GROUPS)
        def _(g):
            rows = xr[k][pl.ds(g * PER_GROUP, PER_GROUP)].astype(jnp.float32).reshape(GROUP_ROWS, width)
            r = pl.ds(pl.multiple_of(g * GROUP_ROWS, GROUP_ROWS), GROUP_ROWS)
            scaled[r, :width] = (rows * gain_ref[:, start:start + width]).astype(jnp.bfloat16)
            square = jnp.sum(rows * rows, axis=-1, keepdims=True)
            square = jnp.broadcast_to(square, (GROUP_ROWS, HEAD))
            squares[r, :] = square if k == 0 else squares[r, :] + square

        @pl.loop(0, FFE // (2 * TILE))
        def _(n):
            for weight, total in ((wg, gate_acc), (wu, up_acc)):
                for half in range(2):
                    c = pl.ds(pl.multiple_of(n * (2 * TILE) + half * TILE, TILE), TILE)
                    new = dot(scaled[:, :width], weight[start:start + width, c])
                    total[:, c] = new if k == 0 else total[:, c] + new

    def remote_count(g):
        return PER_GROUP - (1 if OWN // PER_GROUP == g else 0)

    for g in range(GROUPS):
        mine = slice(g * PER_GROUP, (g + 1) * PER_GROUP)
        lines = slice(g * GROUP_ROWS, (g + 1) * GROUP_ROWS)
        square = squares[lines, 0:1]
        late = []
        for k in range(EARLY, last + 1):
            axis, start, width = PIECES[k]
            wait_for(xr[k].at[pl.ds(g * PER_GROUP, remote_count(g))], group_recv.at[k - EARLY, g])
            rows = xr[k][mine].astype(jnp.float32).reshape(GROUP_ROWS, width)
            square = square + jnp.sum(rows * rows, axis=-1, keepdims=True)
            at_col = (k - EARLY) * 512
            scaled[lines, at_col:at_col + width] = (rows * gain_ref[:, start:start + width]).astype(jnp.bfloat16)
            late.append((at_col, start, width))
        factor = lax.rsqrt(square * (1.0 / WIDTH) + EPS)
        norm = jnp.broadcast_to(factor, (GROUP_ROWS, TILE))
        for n in range(FFE // TILE):
            c = slice(n * TILE, (n + 1) * TILE)
            gate, upper = gate_acc[lines, c], up_acc[lines, c]
            for at_col, start, width in late:
                x = scaled[lines, at_col:at_col + width]
                gate = gate + dot(x, wg[start:start + width, c])
                upper = upper + dot(x, wu[start:start + width, c])
            gate, upper = gate * norm, upper * norm
            hid[:, c] = (gate / (1.0 + jnp.exp(-gate)) * upper).astype(jnp.bfloat16)

        for n in range(WIDTH // TILE):
            c = slice(n * TILE, (n + 1) * TILE)
            result = dot(hid[...], wd[:, c]).astype(jnp.bfloat16)
            ys[mine, :, c] = result.reshape(PER_GROUP, CAP, TILE)

        for i in range(g * PER_GROUP, (g + 1) * PER_GROUP):
            if i == OWN:
                yr[i] = ys[i]
            else:
                a, b = SHIFTS[i]
                remote(ys.at[i], yr.at[i], y_send, y_recv.at[g], at(-a, -b))

    for g in range(GROUPS):
        wait_for(yr.at[pl.ds(g * PER_GROUP, remote_count(g))], y_recv.at[g])

        for n in range(WIDTH // 512):
            c = slice(n * 512, (n + 1) * 512)
            lanes = slice(g * GROUP_ROWS, (g + 1) * GROUP_ROWS)
            got = yr[g * PER_GROUP:(g + 1) * PER_GROUP, :, c].reshape(GROUP_ROWS, 512)
            total = acc[:, c] + dot(mix_hi[:, lanes], got) + dot(mix_lo[:, lanes], got)
            if g < GROUPS - 1:
                acc[:, c] = total
            else:
                out_ref[0, :, c] = total.astype(jnp.bfloat16)

    for t, (src, dst) in enumerate(heads):
        wait_for(dst.at[pl.ds(0, ROWS * (N_SP - 1))], head_send.at[t])
    for i in range(2):
        weight = (proj_a, proj_b)[i]
        wait_for(weight.at[three, half_rows], proj_send.at[i])
        wait_for(weight.at[three, half_rows], relay_send.at[i])
        wait_for(o_buf.at[three], o_send.at[i])
    for k in range(len(PIECES)):
        wait_for(parts[k].at[three], r_send.at[k])
        wait_for(xs[k].at[fifteen], d_send.at[k])
    wait_for(ys.at[fifteen], y_send)


def body(
    queries, keys, values, proj_weight, residual, norm_gain, route, route_weight,
    w_gate, w_up, w_down,
):
    bf16, f32 = jnp.bfloat16, jnp.float32
    vmem = pltpu.VMEM
    dma = pltpu.SemaphoreType.DMA
    anywhere = pl.BlockSpec(memory_space=pl.ANY)
    inside = pl.BlockSpec(memory_space=pltpu.VMEM)
    scratch = [
        vmem((LENGTH, HEAD), bf16), vmem((LENGTH, HEAD), bf16), vmem((LENGTH, HEAD), bf16),
        vmem((LENGTH, LENGTH), bf16), vmem((2 * TILE, HEAD), f32),
        vmem((2, 2 * TILE, TILE), bf16), vmem((2, 2 * TILE, TILE), f32), vmem((TILE, TILE + HEAD), bf16),
        vmem((SIDE, SIDE, ROWS, HEAD), bf16),
        vmem((SIDE, ROWS, 512), bf16), vmem((SIDE, ROWS, 512), bf16),
        vmem((SIDE, ROWS, COLS_Z), bf16), vmem((SIDE, ROWS, COLS_Y), bf16),
    ]
    scratch += [vmem((SIDE, ROWS, width), bf16) for axis, start, width in PIECES] * 2
    scratch += [
        vmem((ROWS, WIDTH), bf16), vmem((ROWS, WIDTH), f32),
        vmem((N_SP * CAP, ROWS), bf16), vmem((ROWS, N_SP * CAP), bf16), vmem((ROWS, N_SP * CAP), bf16),
    ]
    scratch += [vmem((N_SP, CAP, width), bf16) for axis, start, width in PIECES] * 2
    scratch += [
        vmem((N_SP, CAP, WIDTH), bf16), vmem((N_SP, CAP, WIDTH), bf16),
        vmem((N_SP * CAP, 1024), bf16), vmem((N_SP * CAP, HEAD), f32),
        vmem((N_SP * CAP, FFE), f32), vmem((N_SP * CAP, FFE), f32),
        vmem((GROUP_ROWS, FFE), bf16),
        vmem((WIDTH, FFE), bf16), vmem((WIDTH, FFE), bf16), vmem((FFE, WIDTH), bf16),
        dma((6,)), dma((3,)), dma((3,)), dma((2,)), dma((2,)), dma((2,)), dma((2,)),
        dma((2,)), dma((SIDE,)), dma, dma((4,)), dma((4,)),
        dma((4,)), dma((EARLY,)), dma((2, GROUPS)), dma, dma((GROUPS,)),
    ]
    return pl.pallas_call(
        body_kernel,
        out_shape=pltpu.VMEM((1, ROWS, WIDTH), bf16),
        in_specs=[anywhere] * 5 + [inside] * 3 + [anywhere] * 3,
        out_specs=inside,
        scratch_shapes=scratch,
        compiler_params=pltpu.CompilerParams(
            collective_id=0, has_side_effects=True, vmem_limit_bytes=56 * 1024 * 1024
        ),
        name="layer",
    )(
        queries, keys, values, proj_weight, residual, norm_gain.reshape(1, WIDTH),
        jnp.swapaxes(route, 1, 2), jnp.swapaxes(route_weight, 1, 2), w_gate, w_up, w_down,
    )


def solution(mesh):
    return jax.shard_map(
        body,
        mesh=mesh,
        in_specs=(
            P("dp", "sp", None),
            P("dp", "sp", None),
            P("dp", "sp", None),
            P("sp", None),
            P("dp", "sp", None),
            P(),
            P("dp", "sp", None),
            P("dp", "sp", None),
            P("sp", None, None),
            P("sp", None, None),
            P("sp", None, None),
        ),
        out_specs=P("dp", "sp", None),
        check_vma=False,
    )
```

```python
import functools
import math

import jax
import jax.numpy as jnp
from jax import lax
from jax.experimental import pallas as pl
from jax.experimental.pallas import tpu as pltpu
from jax.sharding import PartitionSpec as P

MESH = pl.DeviceIdType.MESH
EPS = 1e-06
SIDE = 4
N_SP = 16
ROWS = 128
HEAD = 128
LENGTH = 2048
WIDTH = 2048
FFE = 1024
COLS_Z = 1024
COLS_Y = WIDTH - COLS_Z
PIECES = (("y", COLS_Z, 512), ("z", 0, 512), ("y", COLS_Z + 512, 512), ("z", 512, 512))
EARLY = 2
CAP = 32
TILE = 256
LOG2E = 1.0 / math.log(2.0)

SHIFTS = (
    (1, 2), (3, 2), (2, 1), (2, 3),
    (2, 2), (2, 0), (0, 2), (0, 0),
    (1, 1), (3, 3), (1, 3), (3, 1),
    (1, 0), (3, 0), (0, 1), (0, 3),
)
OWN = SHIFTS.index((0, 0))
GROUPS = 4
PER_GROUP = 4
GROUP_ROWS = PER_GROUP * CAP


def dot(a, b):
    return jnp.dot(a, b, preferred_element_type=jnp.float32)


def body_kernel(
    q_hbm, k_hbm, v_hbm, proj_hbm, res_hbm, gain_ref, route_ref, rw_ref,
    wg_hbm, wu_hbm, wd_hbm,
    out_ref,
    qh, kh, vh, w_att, carry, softer, power, tri, o_buf, oa, ob, proj_a, proj_b,
    part0, part1, part2, part3, sum0, sum1, sum2, sum3, res, acc, pick, mix_hi, mix_lo,
    xs0, xs1, xs2, xs3, xr0, xr1, xr2, xr3, ys, yr, scaled, squares, gate_acc, up_acc, hid, wg, wu, wd,
    local_sem, head_send, head_recv, proj_send, proj_recv, relay_send, relay_recv,
    o_send, oa_recv, ob_recv, r_send, r_recv, d_send, d_recv, group_recv, y_send, y_recv,
):
    parts, sums = (part0, part1, part2, part3), (sum0, sum1, sum2, sum3)
    xs, xr = (xs0, xs1, xs2, xs3), (xr0, xr1, xr2, xr3)
    me = lax.axis_index("sp")
    dp = lax.axis_index("dp")
    z = me // SIDE
    y = me % SIDE
    core = dp % 2
    partner = dp + 1 - 2 * core

    def at(a, b):
        return ((z + a) % SIDE) * SIDE + (y + b) % SIDE

    others = [s for s in SHIFTS if s != (0, 0)]
    line = (2, 3, 1)

    barrier = pltpu.get_barrier_semaphore()
    for a, b in others:
        pl.semaphore_signal(barrier, inc=1, device_id={"sp": at(a, b)}, device_id_type=MESH)
    pl.semaphore_signal(barrier, inc=1, device_id={"dp": partner}, device_id_type=MESH)

    def local(src, dst, sem):
        copy = pltpu.make_async_copy(src, dst, sem)
        copy.start()
        return copy

    def remote(src, dst, send, recv, peer, axis="sp"):
        pltpu.make_async_remote_copy(
            src_ref=src, dst_ref=dst, send_sem=send, recv_sem=recv,
            device_id={axis: peer}, device_id_type=MESH,
        ).start()

    def wait_for(ref, sem):
        pltpu.make_async_copy(ref, ref, sem).wait()

    my_rows = pl.ds(pl.multiple_of(me * ROWS, ROWS), ROWS)
    core_rows = pl.ds(pl.multiple_of(core * (ROWS // 2), ROWS // 2), ROWS // 2)

    def cols(peer):
        return pl.ds(pl.multiple_of(peer * HEAD, HEAD), HEAD)

    heads = ((k_hbm, kh), (q_hbm, qh), (v_hbm, vh))
    for t, (src, dst) in enumerate(heads):
        local(src.at[0, :, cols(me)], dst.at[my_rows], head_recv.at[t])
    loads = [
        local(proj_hbm.at[:, pl.ds(0, COLS_Z)], proj_a.at[y], local_sem.at[4]),
        local(proj_hbm.at[:, pl.ds(COLS_Z, COLS_Y)], proj_b.at[z], local_sem.at[5]),
    ]

    pl.semaphore_wait(barrier, N_SP)

    def send_heads(t, a, b):
        src, dst = heads[t]
        peer = at(a, b)
        remote(src.at[0, :, cols(peer)], dst.at[my_rows], head_send.at[t], head_recv.at[t], peer)

    for t in range(3):
        for a, b in others:
            send_heads(t, a, b)
    for s in line:
        remote(proj_hbm.at[core_rows, pl.ds(0, COLS_Z)], proj_a.at[y, core_rows],
               proj_send.at[0], proj_recv.at[0], at(0, s))
    for s in line:
        remote(proj_hbm.at[core_rows, pl.ds(COLS_Z, COLS_Y)], proj_b.at[z, core_rows],
               proj_send.at[1], proj_recv.at[1], at(s, 0))
    loads += [
        local(res_hbm.at[0], res, local_sem.at[0]),
        local(wg_hbm.at[0], wg, local_sem.at[1]),
        local(wu_hbm.at[0], wu, local_sem.at[2]),
        local(wd_hbm.at[0], wd, local_sem.at[3]),
    ]

    j = lax.broadcasted_iota(jnp.int32, (TILE, TILE + HEAD), 0)
    s = lax.broadcasted_iota(jnp.int32, (TILE, TILE + HEAD), 1)
    tri[...] = jnp.where((j > s) | (s >= TILE), 1.0, 0.0).astype(jnp.bfloat16)

    @pl.loop(0, LENGTH // 64)
    def _(i):
        w_att[pl.ds(pl.multiple_of(i * 64, 64), 64), :] = jnp.zeros((64, LENGTH), jnp.bfloat16)

    slots = N_SP * CAP
    lane = lax.broadcasted_iota(jnp.int32, (ROWS, slots), 1)
    place = lane // CAP
    expert = jnp.zeros((ROWS, slots), jnp.int32)
    for i, (a, b) in enumerate(SHIFTS):
        expert = jnp.where(place == i, at(a, b), expert)
    zeros = jnp.zeros((6, ROWS), jnp.float32)
    route = jnp.concatenate([route_ref[0].astype(jnp.float32), zeros], axis=0).T
    share = jnp.concatenate([rw_ref[0], zeros], axis=0).T
    expert = expert.astype(jnp.float32)
    first = route[:, 0:1] == expert
    second = route[:, 1:2] == expert
    named = jnp.where(first | second, 1.0, 0.0)
    r0 = lax.broadcasted_iota(jnp.int32, (ROWS, ROWS), 0)
    r1 = lax.broadcasted_iota(jnp.int32, (ROWS, ROWS), 1)
    before = jnp.where(r1 < r0, 1.0, 0.0).astype(jnp.bfloat16)
    slot = dot(before, named.astype(jnp.bfloat16))
    held = jnp.where(slot == (lane - place * CAP).astype(jnp.float32), named, 0.0)
    pick[...] = held.T.astype(jnp.bfloat16)
    mix = held * jnp.where(first, share[:, 0:1], share[:, 1:2])
    high = mix.astype(jnp.bfloat16)
    mix_hi[...] = high
    mix_lo[...] = (mix - high.astype(jnp.float32)).astype(jnp.bfloat16)

    wait_for(kh, head_recv.at[0])
    wait_for(qh, head_recv.at[1])
    scale = HEAD ** (-0.5)

    causal = lax.broadcasted_iota(jnp.int32, (TILE, TILE), 1) < lax.broadcasted_iota(
        jnp.int32, (TILE, TILE), 0
    )

    def soften(base, lines, k0, which, diagonal):
        rows = slice(*lines)
        u = lax.dot_general(
            qh[pl.ds(pl.multiple_of(base + lines[0], TILE), lines[1] - lines[0]), :],
            kh[pl.ds(k0, TILE), :], (((1,), (1,)), ((), ())),
            preferred_element_type=jnp.float32,
        ) * scale
        low = jnp.log(1.0 + jnp.exp2(jnp.abs(u) * -LOG2E))
        soft = jnp.maximum(u, 0.0) + low
        if diagonal:
            soft = jnp.where(causal, soft, 0.0)
        softer[which, rows, :] = soft.astype(jnp.bfloat16)
        power[which, rows, :] = jnp.minimum(u, 0.0) - low

    def weigh(base, lines, k0, which, diagonal, fresh):
        rows = slice(*lines)
        sums = dot(softer[which, rows, :], tri[...])
        less = sums[:, :TILE]
        total = sums[:, TILE:]
        if not fresh:
            later = carry[rows, :]
            less = less + jnp.concatenate([later, later], axis=1)
            total = total + later
        weight = jnp.exp2((power[which, rows, :] - less) * LOG2E)
        if diagonal:
            weight = jnp.where(causal, weight, 0.0)
        place = pl.ds(pl.multiple_of(base + lines[0], TILE), lines[1] - lines[0])
        w_att[place, pl.ds(k0, TILE)] = weight.astype(jnp.bfloat16)
        carry[rows, :] = total

    upper, lower, both = (0, TILE), (TILE, 2 * TILE), (0, 2 * TILE)

    def quarter_weights(quarter):
        base = pl.multiple_of(quarter * 512, 512)
        second = pl.multiple_of(base + TILE, TILE)
        soften(base, lower, second, 1, True)
        soften(base, upper, base, 0, True)
        soften(base, lower, base, 0, False)
        weigh(base, lower, second, 1, True, True)
        weigh(base, upper, base, 0, True, True)
        weigh(base, lower, base, 0, False, False)

        @pl.loop(0, quarter)
        def _(i):
            for which in range(2):
                k0 = pl.multiple_of((2 * quarter - 2 * i - 1 - which) * TILE, TILE)
                soften(base, both, k0, which, False)
                weigh(base, both, k0, which, False, False)

    def quarter_values(i):
        quarter = (z + 1 + i) % SIDE
        rows = pl.ds(pl.multiple_of(quarter * 512, 512), 512)
        o_buf[quarter] = dot(w_att[rows, :], vh[...]).astype(jnp.bfloat16).reshape(SIDE, ROWS, HEAD)
        if i < SIDE - 1:
            remote(o_buf.at[quarter], ob.at[:, :, cols(z)], o_send.at[1], ob_recv, quarter * SIDE + y)
        else:
            ob[:, :, cols(z)] = o_buf[z]
        for s in line:
            peer_y = (y + s) % SIDE
            remote(o_buf.at[quarter, peer_y], oa.at[quarter, :, cols(y)], o_send.at[0],
                   oa_recv.at[quarter], z * SIDE + peer_y)
        oa[quarter, :, cols(y)] = o_buf[quarter, y]

    three = pl.ds(0, SIDE - 1)
    half_rows = pl.ds(0, ROWS // 2)

    def relay():
        for index, (weight, mine) in enumerate(((proj_a, y), (proj_b, z))):
            wait_for(weight.at[three, half_rows], proj_recv.at[index])
            for s in line:
                piece = weight.at[(mine + s) % SIDE, core_rows]
                remote(piece, piece, relay_send.at[index], relay_recv.at[index], partner, "dp")

    def project_z(i):
        quarter = (z + 1 + i) % SIDE
        wait_for(oa.at[0, :, pl.ds(0, 3 * HEAD)], oa_recv.at[quarter])
        left = oa[quarter]
        for k, (axis, start, width) in enumerate(PIECES):
            if axis == "y":
                continue
            for n in range(width // TILE):
                right = proj_a[:, :, start + n * TILE:start + (n + 1) * TILE].reshape(512, TILE)
                parts[k][quarter, :, n * TILE:(n + 1) * TILE] = dot(left, right).astype(jnp.bfloat16)
            if i < SIDE - 1:
                remote(parts[k].at[quarter], sums[k].at[z], r_send.at[k], r_recv.at[k], quarter * SIDE + y)
            else:
                sums[k][z] = parts[k][z]

    def project_y(k):
        start, width = PIECES[k][1] - COLS_Z, PIECES[k][2]
        for n in range(width // TILE):
            right = proj_b[:, :, start + n * TILE:start + (n + 1) * TILE].reshape(512, TILE)
            block = dot(ob[...].reshape(512, 512), right).astype(jnp.bfloat16)
            parts[k][:, :, n * TILE:(n + 1) * TILE] = block.reshape(SIDE, ROWS, TILE)
        for s in line:
            peer_y = (y + s) % SIDE
            remote(parts[k].at[peer_y], sums[k].at[y], r_send.at[k], r_recv.at[k], z * SIDE + peer_y)
        sums[k][y] = parts[k][y]

    quarter_weights((z + 1) % SIDE)
    quarter_weights((z + 2) % SIDE)
    wait_for(vh, head_recv.at[2])
    quarter_values(0)
    quarter_values(1)
    quarter_weights((z + 3) % SIDE)
    quarter_values(2)
    relay()
    quarter_weights(z)
    quarter_values(3)
    loads[0].wait()
    loads[1].wait()
    wait_for(proj_b.at[three, half_rows], relay_recv.at[1])
    wait_for(ob.at[:, :, pl.ds(0, 3 * HEAD)], ob_recv)
    project_y(0)
    wait_for(proj_a.at[three, half_rows], relay_recv.at[0])
    project_z(0)
    project_y(2)
    project_z(1)
    project_z(2)
    project_z(3)

    last = len(PIECES) - 1

    def dispatch(k, g, sem):
        for i in range(g * PER_GROUP, (g + 1) * PER_GROUP):
            if i != OWN:
                remote(xs[k].at[i], xr[k].at[i], d_send.at[k], sem, at(*SHIFTS[i]))

    loads[2].wait()
    for k, (axis, start, width) in enumerate(PIECES):
        wait_for(sums[k].at[three], r_recv.at[k])
        for n in range(width // TILE):
            c = slice(n * TILE, (n + 1) * TILE)
            place = slice(start + n * TILE, start + (n + 1) * TILE)
            total = res[:, place].astype(jnp.float32)
            for i in range(SIDE):
                total = total + sums[k][i, :, c].astype(jnp.float32)
            stream = total.astype(jnp.bfloat16)
            acc[:, place] = stream.astype(jnp.float32)
            rows = dot(pick[...], stream).astype(jnp.bfloat16)
            xs[k][:, :, c] = rows.reshape(N_SP, CAP, TILE)
        if k < EARLY:
            for g in range(GROUPS):
                dispatch(k, g, d_recv.at[k])
        xr[k][OWN] = xs[k][OWN]
        if k == EARLY:
            dispatch(k, 0, group_recv.at[k - EARLY, 0])
    for g in range(GROUPS):
        for k in range(EARLY, last + 1):
            if g > 0 or k > EARLY:
                dispatch(k, g, group_recv.at[k - EARLY, g])

    for load in loads[3:]:
        load.wait()
    fifteen = pl.ds(0, N_SP - 1)
    for k, (axis, start, width) in enumerate(PIECES[:EARLY]):
        wait_for(xr[k].at[fifteen], d_recv.at[k])

        @pl.loop(0, GROUPS)
        def _(g):
            rows = xr[k][pl.ds(g * PER_GROUP, PER_GROUP)].astype(jnp.float32).reshape(GROUP_ROWS, width)
            r = pl.ds(pl.multiple_of(g * GROUP_ROWS, GROUP_ROWS), GROUP_ROWS)
            scaled[r, :width] = (rows * gain_ref[:, start:start + width]).astype(jnp.bfloat16)
            square = jnp.sum(rows * rows, axis=-1, keepdims=True)
            square = jnp.broadcast_to(square, (GROUP_ROWS, HEAD))
            squares[r, :] = square if k == 0 else squares[r, :] + square

        @pl.loop(0, FFE // (2 * TILE))
        def _(n):
            for weight, total in ((wg, gate_acc), (wu, up_acc)):
                for half in range(2):
                    c = pl.ds(pl.multiple_of(n * (2 * TILE) + half * TILE, TILE), TILE)
                    new = dot(scaled[:, :width], weight[start:start + width, c])
                    total[:, c] = new if k == 0 else total[:, c] + new

    def remote_count(g):
        return PER_GROUP - (1 if OWN // PER_GROUP == g else 0)

    for g in range(GROUPS):
        mine = slice(g * PER_GROUP, (g + 1) * PER_GROUP)
        lines = slice(g * GROUP_ROWS, (g + 1) * GROUP_ROWS)
        square = squares[lines, 0:1]
        late = []
        for k in range(EARLY, last + 1):
            axis, start, width = PIECES[k]
            wait_for(xr[k].at[pl.ds(g * PER_GROUP, remote_count(g))], group_recv.at[k - EARLY, g])
            rows = xr[k][mine].astype(jnp.float32).reshape(GROUP_ROWS, width)
            square = square + jnp.sum(rows * rows, axis=-1, keepdims=True)
            at_col = (k - EARLY) * 512
            scaled[lines, at_col:at_col + width] = (rows * gain_ref[:, start:start + width]).astype(jnp.bfloat16)
            late.append((at_col, start, width))
        factor = lax.rsqrt(square * (1.0 / WIDTH) + EPS)
        norm = jnp.broadcast_to(factor, (GROUP_ROWS, TILE))
        for n in range(FFE // TILE):
            c = slice(n * TILE, (n + 1) * TILE)
            gate, upper = gate_acc[lines, c], up_acc[lines, c]
            for at_col, start, width in late:
                x = scaled[lines, at_col:at_col + width]
                gate = gate + dot(x, wg[start:start + width, c])
                upper = upper + dot(x, wu[start:start + width, c])
            gate, upper = gate * norm, upper * norm
            hid[:, c] = (gate / (1.0 + jnp.exp(-gate)) * upper).astype(jnp.bfloat16)

        for n in range(WIDTH // TILE):
            c = slice(n * TILE, (n + 1) * TILE)
            result = dot(hid[...], wd[:, c]).astype(jnp.bfloat16)
            ys[mine, :, c] = result.reshape(PER_GROUP, CAP, TILE)

        for i in range(g * PER_GROUP, (g + 1) * PER_GROUP):
            if i == OWN:
                yr[i] = ys[i]
            else:
                a, b = SHIFTS[i]
                remote(ys.at[i], yr.at[i], y_send, y_recv.at[g], at(-a, -b))

    for g in range(GROUPS):
        wait_for(yr.at[pl.ds(g * PER_GROUP, remote_count(g))], y_recv.at[g])

        for n in range(WIDTH // 512):
            c = slice(n * 512, (n + 1) * 512)
            lanes = slice(g * GROUP_ROWS, (g + 1) * GROUP_ROWS)
            got = yr[g * PER_GROUP:(g + 1) * PER_GROUP, :, c].reshape(GROUP_ROWS, 512)
            total = acc[:, c] + dot(mix_hi[:, lanes], got) + dot(mix_lo[:, lanes], got)
            if g < GROUPS - 1:
                acc[:, c] = total
            else:
                out_ref[0, :, c] = total.astype(jnp.bfloat16)

    for t, (src, dst) in enumerate(heads):
        wait_for(dst.at[pl.ds(0, ROWS * (N_SP - 1))], head_send.at[t])
    for i in range(2):
        weight = (proj_a, proj_b)[i]
        wait_for(weight.at[three, half_rows], proj_send.at[i])
        wait_for(weight.at[three, half_rows], relay_send.at[i])
        wait_for(o_buf.at[three], o_send.at[i])
    for k in range(len(PIECES)):
        wait_for(parts[k].at[three], r_send.at[k])
        wait_for(xs[k].at[fifteen], d_send.at[k])
    wait_for(ys.at[fifteen], y_send)


def body(
    queries, keys, values, proj_weight, residual, norm_gain, route, route_weight,
    w_gate, w_up, w_down,
):
    bf16, f32 = jnp.bfloat16, jnp.float32
    vmem = pltpu.VMEM
    dma = pltpu.SemaphoreType.DMA
    anywhere = pl.BlockSpec(memory_space=pl.ANY)
    inside = pl.BlockSpec(memory_space=pltpu.VMEM)
    scratch = [
        vmem((LENGTH, HEAD), bf16), vmem((LENGTH, HEAD), bf16), vmem((LENGTH, HEAD), bf16),
        vmem((LENGTH, LENGTH), bf16), vmem((2 * TILE, HEAD), f32),
        vmem((2, 2 * TILE, TILE), bf16), vmem((2, 2 * TILE, TILE), f32), vmem((TILE, TILE + HEAD), bf16),
        vmem((SIDE, SIDE, ROWS, HEAD), bf16),
        vmem((SIDE, ROWS, 512), bf16), vmem((SIDE, ROWS, 512), bf16),
        vmem((SIDE, ROWS, COLS_Z), bf16), vmem((SIDE, ROWS, COLS_Y), bf16),
    ]
    scratch += [vmem((SIDE, ROWS, width), bf16) for axis, start, width in PIECES] * 2
    scratch += [
        vmem((ROWS, WIDTH), bf16), vmem((ROWS, WIDTH), f32),
        vmem((N_SP * CAP, ROWS), bf16), vmem((ROWS, N_SP * CAP), bf16), vmem((ROWS, N_SP * CAP), bf16),
    ]
    scratch += [vmem((N_SP, CAP, width), bf16) for axis, start, width in PIECES] * 2
    scratch += [
        vmem((N_SP, CAP, WIDTH), bf16), vmem((N_SP, CAP, WIDTH), bf16),
        vmem((N_SP * CAP, 1024), bf16), vmem((N_SP * CAP, HEAD), f32),
        vmem((N_SP * CAP, FFE), f32), vmem((N_SP * CAP, FFE), f32),
        vmem((GROUP_ROWS, FFE), bf16),
        vmem((WIDTH, FFE), bf16), vmem((WIDTH, FFE), bf16), vmem((FFE, WIDTH), bf16),
        dma((6,)), dma((3,)), dma((3,)), dma((2,)), dma((2,)), dma((2,)), dma((2,)),
        dma((2,)), dma((SIDE,)), dma, dma((4,)), dma((4,)),
        dma((4,)), dma((EARLY,)), dma((2, GROUPS)), dma, dma((GROUPS,)),
    ]
    return pl.pallas_call(
        body_kernel,
        out_shape=pltpu.VMEM((1, ROWS, WIDTH), bf16),
        in_specs=[anywhere] * 5 + [inside] * 3 + [anywhere] * 3,
        out_specs=inside,
        scratch_shapes=scratch,
        compiler_params=pltpu.CompilerParams(
            collective_id=0, has_side_effects=True, vmem_limit_bytes=56 * 1024 * 1024
        ),
        name="layer",
    )(
        queries, keys, values, proj_weight, residual, norm_gain.reshape(1, WIDTH),
        jnp.swapaxes(route, 1, 2), jnp.swapaxes(route_weight, 1, 2), w_gate, w_up, w_down,
    )


def solution(mesh):
    return jax.shard_map(
        body,
        mesh=mesh,
        in_specs=(
            P("dp", "sp", None),
            P("dp", "sp", None),
            P("dp", "sp", None),
            P("sp", None),
            P("dp", "sp", None),
            P(),
            P("dp", "sp", None),
            P("dp", "sp", None),
            P("sp", None, None),
            P("sp", None, None),
            P("sp", None, None),
        ),
        out_specs=P("dp", "sp", None),
        check_vma=False,
    )
```
